512 devices in a mesh: ep: 128 (over z, y, core), tp: 4 (over x).
Axes of the slice: x: 4, y: 8, z: 8, core: 2. Of those that a mesh axis runs over, the one named last changes fastest.
Arguments:
- tokens: bfloat16 [2048, 1024], P(('ep', 'tp')), may hold values from -6 to 6
- gain_attn: bfloat16 [1024], replicated, may hold values from 0.099609375 to 1.8984375
- gain_ffn: bfloat16 [1024], replicated, may hold values from 0.099609375 to 1.8984375
- w_query: bfloat16 [1024, 512], P(None, 'tp'), may hold values from -0.1875 to 0.1875
- w_key: bfloat16 [1024, 128], replicated, may hold values from -0.1875 to 0.1875
- w_value: bfloat16 [1024, 128], replicated, may hold values from -0.1875 to 0.1875
- w_output: bfloat16 [512, 1024], P('tp'), may hold values from -0.25 to 0.25
- head_bias: float32 [8], replicated, may hold values from -9 to -2
- keys_cache: bfloat16 [2048, 1024, 128], P(('ep', 'tp')), may hold values from -6 to 6
- values_cache: bfloat16 [2048, 1024, 128], P(('ep', 'tp')), may hold values from -6 to 6
- lengths: int32 [2048], P(('ep', 'tp')), may hold values from 256 to 1024
- dense_gate_w: bfloat16 [4096, 1024], P('ep'), may hold values from -0.1875 to 0.1875
- dense_up_w: bfloat16 [4096, 1024], P('ep'), may hold values from -0.1875 to 0.1875
- dense_down_w: bfloat16 [4096, 1024], P('ep'), may hold values from -0.09375 to 0.09375
- mix_gate: bfloat16 [1024], replicated, may hold values from -0.1875 to 0.1875
- expert_gate: bfloat16 [128, 1024, 1024], P('ep', None, 'tp'), may hold values from -0.1875 to 0.1875
- expert_up: bfloat16 [128, 1024, 1024], P('ep', None, 'tp'), may hold values from -0.1875 to 0.1875
- expert_down: bfloat16 [128, 1024, 1024], P('ep', 'tp'), may hold values from -0.09375 to 0.09375
- routes: int32 [2048, 2], P(('ep', 'tp')), may hold values from 0 to 31, all different within a row; in each aligned block of 16 rows (0 to 15, 16 to 31, ...) at most 2 rows name the same one
- route_weights: float32 [2048, 2], P(('ep', 'tp')), may hold values from 0.1 to 0.9
Outputs:
- layer_out: bfloat16 [2048, 1024], P(('ep', 'tp'))
- new_keys: bfloat16 [2048, 128], P(('ep', 'tp'))
- new_values: bfloat16 [2048, 128], P(('ep', 'tp'))
The draws below stay inside these ranges and needn't reach their ends.
Inputs may be any that keep to these rules, and one draw needn't show every extreme that they name: `routes`: each row names 2 different experts. In each aligned block of 16 rows (the tokens held by one index of ep) no expert is named by more than 2 rows, a bound that some block reaches.
All inputs are finite; a program needn't handle non-finite values.
Results may differ from the reference program's by a relative error of at most 0.01.
Values may be sent and summed in bfloat16 or wider, within the bound.
No kernel may reach another device: no remote copies, remote signals or barrier semaphores. Data moves between devices by JAX's collectives and lax.ppermute only.
A program may use at most 64 MiB of HBM per device.

```python
import math
import jax
import jax.numpy as jnp
import numpy as np
from jax import lax

D = 1024
HEADS = 8
KV_HEADS = 2
HEAD = 64
FF_EXP = 4096
DENSE_FF = 4096
TOP = 2
SPLIT = 4
CACHE = 1024
GROUP = 16
SEQS = 2048
EXPERTS = 32
CAP = 2


def touch_ends(array, stream_key, least, high):
    shape = array.shape
    spot = [jax.random.randint(jax.random.fold_in(stream_key, axis), (), 0, shape[axis]) for axis in range(len(shape))]
    array = array.at[tuple(spot)].set(least)
    longest = shape.index(max(shape))
    spot[longest] = (spot[longest] + 1) % shape[longest]
    return array.at[tuple(spot)].set(high)


def shard_levels(own_key, dims, pieces, least, high):
    loudness = 1.0
    for dim, shards_of in pieces:
        draws = jax.random.uniform(jax.random.fold_in(jax.random.fold_in(own_key, 6), dim), (shards_of,), jnp.float32, least / len(pieces), high / len(pieces))
        loudness = loudness * jnp.repeat(jnp.exp(draws), dims[dim] // shards_of).reshape((-1,) + (1,) * (len(dims) - 1 - dim))
    return loudness


def shared_out(stream_key, own, number, rows, amount, top, reach, slope):
    ranking = jax.random.permutation(stream_key, amount)
    packed, ordinary = shares(amount, rows * top, reach, slope, True), shares(amount, rows * top, reach, slope, False)
    places = jnp.arange(amount)

    def named(sizes, turn):
        used = int((sizes > 0).sum())
        fixed = max(1, used // 4)
        shifted = fixed + (places - fixed + turn * (used - fixed)) % max(1, amount - fixed)
        return jnp.zeros((amount,), jnp.int32).at[ranking[jnp.where(places < fixed, places, shifted)]].set(jnp.asarray(sizes, jnp.int32))

    sizes = jnp.where(number % 4 == 0, named(packed, number // 4), named(ordinary, number - number // 4 - 1))
    mixed = jax.random.permutation(jax.random.fold_in(own, 3), amount)
    donor, taker = mixed[0:amount // 2 * 2:2], mixed[1:amount // 2 * 2:2]
    slack = jnp.minimum(sizes[donor] - 1, reach - sizes[taker]) // 2
    slack = jnp.where((donor == ranking[0]) | (taker == ranking[0]) | (sizes[taker] == 0), 0, jnp.maximum(slack, 0))
    shifted = jax.random.randint(jax.random.fold_in(own, 4), (amount // 2,), 0, 1 << 20) % (slack + 1)
    sizes = sizes.at[donor].add(-shifted).at[taker].add(shifted)
    members = jnp.searchsorted(jnp.cumsum(sizes), jnp.arange(rows * top), side="right").astype(jnp.int32)
    listing = members.reshape(top, rows).T
    listing = listing[jax.random.permutation(jax.random.fold_in(own, 1), rows)]
    turn = jax.random.randint(jax.random.fold_in(own, 2), (rows, 1), 0, top)
    return jnp.take_along_axis(listing, (jnp.arange(top)[None, :] + turn) % top, axis=1)


def shares(amount, total, most, skew, full):
    portions = [(1 << 20) // math.isqrt(rank ** skew) + 1 for rank in range(1, amount + 1)]
    largest = most if full else min(most, max(-(-total // amount), total * portions[0] // sum(portions)))
    least = 1 if total - largest >= amount - 1 else 0
    given, surplus = [largest] + [least] * (amount - 1), total - largest - least * (amount - 1)
    while surplus > 0:
        candidates = [i for i in range(1, amount) if given[i] < largest] or [i for i in range(1, amount) if given[i] < most]
        pool, left = sum([portions[i] for i in candidates]), surplus
        for i in candidates:
            addition = min(most - given[i], max(1, left * portions[i] // pool), surplus)
            given[i] = given[i] + addition
            surplus = surplus - addition
    return np.array(given)


def centred(key, dims, deviation, bound, split=(), held_as=jnp.bfloat16):
    array = deviation * jax.random.normal(key, dims, jnp.float32)
    if split:
        array = array * shard_levels(key, dims, split, -0.22, 0.18)
    return jnp.clip(array, -bound, bound).astype(held_as)


def setup_inputs(seed: int = 0) -> dict:
    key_list = jax.random.split(jax.random.key(seed), 21)
    tokens = centred(key_list[0], (SEQS, D), 1.0, 6.0, ((0, 512),))
    gain_attn = jnp.clip(1.0 + 0.18 * jax.random.normal(key_list[1], (D,), jnp.float32), 0.099609375, 1.8984375).astype(jnp.bfloat16)
    gain_ffn = jnp.clip(1.0 + 0.18 * jax.random.normal(key_list[2], (D,), jnp.float32), 0.099609375, 1.8984375).astype(jnp.bfloat16)
    w_query = centred(key_list[3], (D, HEADS * HEAD), D ** -0.5, 0.1875, ((1, 4),))
    w_key = centred(key_list[4], (D, KV_HEADS * HEAD), D ** -0.5, 0.1875)
    w_value = centred(key_list[5], (D, KV_HEADS * HEAD), D ** -0.5, 0.1875)
    w_output = centred(key_list[6], (HEADS * HEAD, D), (HEADS * HEAD) ** -0.5, 0.25, ((0, 4),))
    head_bias = jnp.clip(jax.random.uniform(key_list[7], (HEADS,), jnp.float32, -9.0, -2.0), -9.0, -2.0)
    keys_cache = centred(key_list[8], (SEQS, CACHE, KV_HEADS * HEAD), 1.0, 6.0, ((0, 512),))
    values_cache = centred(key_list[9], (SEQS, CACHE, KV_HEADS * HEAD), 1.0, 6.0, ((0, 512),))
    lengths = touch_ends(jax.random.randint(key_list[10], (SEQS,), CACHE // 4, CACHE + 1), jax.random.fold_in(key_list[10], 1), CACHE // 4, CACHE).astype(jnp.int32)
    dense_gate_w = centred(key_list[11], (DENSE_FF, D), D ** -0.5, 0.1875, ((0, 128),))
    dense_up_w = centred(key_list[12], (DENSE_FF, D), D ** -0.5, 0.1875, ((0, 128),))
    dense_down_w = centred(key_list[13], (DENSE_FF, D), DENSE_FF ** -0.5, 0.09375, ((0, 128),))
    mix_gate = centred(key_list[14], (D,), D ** -0.5, 0.1875)
    expert_gate = centred(key_list[15], (EXPERTS * SPLIT, D, FF_EXP // SPLIT), D ** -0.5, 0.1875, ((0, 128), (2, 4)))
    expert_up = centred(key_list[16], (EXPERTS * SPLIT, D, FF_EXP // SPLIT), D ** -0.5, 0.1875, ((0, 128), (2, 4)))
    expert_down = centred(key_list[17], (EXPERTS * SPLIT, FF_EXP // SPLIT, D), FF_EXP ** -0.5, 0.09375, ((0, 128), (1, 4)))
    routes_keys = jax.random.split(jax.random.fold_in(key_list[18], 1), SEQS // GROUP)
    routes_turns = jax.random.permutation(jax.random.fold_in(key_list[18], 3), SEQS // GROUP)
    routes = jax.vmap(lambda own, number: shared_out(jax.random.fold_in(key_list[18], 2), own, number, GROUP, EXPERTS, TOP, CAP, 2))(routes_keys, routes_turns).reshape((SEQS, TOP))
    route_weights = jnp.clip(0.1 + 0.79999997 * jax.random.uniform(key_list[19], (SEQS, TOP), jnp.float32) ** shard_levels(key_list[19], (SEQS, TOP), ((0, 512),), -0.2, 0.2), 0.1, 0.9)
    return dict(tokens=tokens, gain_attn=gain_attn, gain_ffn=gain_ffn, w_query=w_query, w_key=w_key, w_value=w_value, w_output=w_output, head_bias=head_bias, keys_cache=keys_cache, values_cache=values_cache, lengths=lengths, dense_gate_w=dense_gate_w, dense_up_w=dense_up_w, dense_down_w=dense_down_w, mix_gate=mix_gate, expert_gate=expert_gate, expert_up=expert_up, expert_down=expert_down, routes=routes, route_weights=route_weights)


EPS = 1e-06

def settle(values):
    return lax.optimization_barrier(values).astype(jnp.float32)

def rms_scale(values, gains):
    widened = settle(values)
    scaled = widened * lax.rsqrt(lax.optimization_barrier(jnp.mean(widened * widened, axis=-1, keepdims=True)) + EPS)
    return (scaled * gains.astype(jnp.float32)).astype(jnp.bfloat16)

def slot_table(route_ids, experts_total, capacity):
    expert_ids = lax.broadcasted_iota(jnp.int32, route_ids.shape + (experts_total,), route_ids.ndim)
    picked = (route_ids[..., None] == expert_ids).astype(jnp.float32)
    chosen = lax.optimization_barrier(jnp.sum(picked, axis=-2))
    earlier = jnp.cumsum(chosen, axis=-2) - chosen
    slot_ids = lax.broadcasted_iota(jnp.int32, chosen.shape + (capacity,), chosen.ndim).astype(jnp.float32)
    table = chosen[..., None] * (earlier[..., None] == slot_ids).astype(jnp.float32)
    return (picked, table)

def stick_read(queries, keys_cache, values_cache, lengths, head_bias):
    seq_count, positions, joined = keys_cache.shape
    kv_heads = joined // HEAD
    groups = HEADS // kv_heads
    query_heads = settle(queries).reshape(seq_count, kv_heads, groups, HEAD)
    key_heads = keys_cache.astype(jnp.float32).reshape(seq_count, positions, kv_heads, HEAD)
    value_heads = values_cache.astype(jnp.float32).reshape(seq_count, positions, kv_heads, HEAD)
    scores = jnp.einsum('bkgd,bpkd->bkgp', query_heads, key_heads)
    scores = scores * (1.0 / math.sqrt(HEAD)) + head_bias.reshape(1, kv_heads, groups, 1)
    position = lax.broadcasted_iota(jnp.int32, scores.shape, 3)
    is_live = position < lengths.reshape(seq_count, 1, 1, 1)
    skipped = jnp.where(is_live, jax.nn.log_sigmoid(-scores), 0.0)
    later_sum = lax.cumsum(skipped, axis=3, reverse=True) - skipped
    weights = jnp.where(is_live, jnp.exp(jax.nn.log_sigmoid(scores) + later_sum), 0.0).astype(jnp.bfloat16)
    mixed_heads = jnp.einsum('bkgp,bpkd->bkgd', settle(weights), value_heads)
    return mixed_heads.astype(jnp.bfloat16).reshape(seq_count, HEADS * HEAD)

def reference(tokens, gain_attn, gain_ffn, w_query, w_key, w_value, w_output, head_bias, keys_cache, values_cache, lengths, dense_gate_w, dense_up_w, dense_down_w, mix_gate, expert_gate, expert_up, expert_down, routes, route_weights):
    seq_total = tokens.shape[0]
    blocks = seq_total // GROUP
    attn_in = rms_scale(tokens, gain_attn)
    queries = jnp.dot(attn_in, w_query, preferred_element_type=jnp.float32).astype(jnp.bfloat16)
    new_keys = jnp.dot(attn_in, w_key, preferred_element_type=jnp.float32).astype(jnp.bfloat16)
    new_values = jnp.dot(attn_in, w_value, preferred_element_type=jnp.float32).astype(jnp.bfloat16)

    def read_block(inputs):
        return stick_read(inputs[0], inputs[1], inputs[2], inputs[3], head_bias)
    mixed_heads = lax.map(read_block, (queries.reshape(blocks, GROUP, HEADS * HEAD), keys_cache.reshape(blocks, GROUP, CACHE, KV_HEADS * HEAD), values_cache.reshape(blocks, GROUP, CACHE, KV_HEADS * HEAD), lengths.reshape(blocks, GROUP)))
    mixed_heads = mixed_heads.reshape(seq_total, HEADS * HEAD)
    attn_sum = jnp.dot(mixed_heads, w_output, preferred_element_type=jnp.float32)
    residual = (tokens.astype(jnp.float32) + attn_sum).astype(jnp.bfloat16)
    ffn_in = rms_scale(residual, gain_ffn)
    mix_scale = jax.nn.sigmoid(jnp.dot(ffn_in, mix_gate, preferred_element_type=jnp.float32))
    gate_dense = jnp.dot(ffn_in, dense_gate_w.T, preferred_element_type=jnp.float32)
    up_dense = jnp.dot(ffn_in, dense_up_w.T, preferred_element_type=jnp.float32)
    hidden_dense = (jax.nn.silu(gate_dense) * up_dense).astype(jnp.bfloat16)
    dense_out = jnp.dot(hidden_dense, dense_down_w, preferred_element_type=jnp.float32)
    grouped = settle(ffn_in).reshape(blocks, GROUP, D)
    picked, table = slot_table(routes.reshape(blocks, GROUP, TOP), EXPERTS, CAP)
    weight_of = lax.optimization_barrier(jnp.sum(route_weights.reshape(blocks, GROUP, TOP)[..., None] * picked, axis=2))

    def one_expert(index):
        slots = lax.dynamic_index_in_dim(table, index, 2, keepdims=False)
        rows = jnp.einsum('njc,njd->ncd', slots, grouped).reshape(blocks * CAP, D)
        first = index * SPLIT
        gate_block = lax.dynamic_slice_in_dim(expert_gate, first, SPLIT, 0).astype(jnp.float32)
        up_block = lax.dynamic_slice_in_dim(expert_up, first, SPLIT, 0).astype(jnp.float32)
        down_block = lax.dynamic_slice_in_dim(expert_down, first, SPLIT, 0).astype(jnp.float32)
        gate_val = jnp.einsum('rd,sdu->rsu', rows, gate_block)
        up_val = jnp.einsum('rd,sdu->rsu', rows, up_block)
        hidden = settle((jax.nn.silu(gate_val) * up_val).astype(jnp.bfloat16))
        return jnp.einsum('rsu,sud->rd', hidden, down_block).reshape(blocks, CAP, D)
    expert_outs = lax.map(one_expert, jnp.arange(EXPERTS, dtype=jnp.int32))
    moe_out = jnp.einsum('njxc,xncd->njd', table * weight_of[..., None], expert_outs, precision=lax.Precision.HIGHEST).reshape(seq_total, D)
    layer_out = (settle(residual) + moe_out + mix_scale[:, None] * dense_out).astype(jnp.bfloat16)
    return (layer_out, new_keys, new_values)
```

```python
import functools
import math

import jax
import jax.numpy as jnp
from jax import lax
from jax.experimental import pallas as pl
from jax.experimental.pallas import tpu as pltpu
from jax.sharding import Mesh, PartitionSpec as P

HEADS = 8
KV = 2
HEAD = 64
EPS = 1e-06
D = 1024
HALF = D // 2
CACHE = 1024
OWN = 4
TP = 4
CHIPS = 64
MSG = 8
ROWS = CHIPS * MSG
F32 = jnp.float32
BF16 = jnp.bfloat16


VMEM = pl.BlockSpec(memory_space=pltpu.VMEM)
SMEM = pl.BlockSpec(memory_space=pltpu.SMEM)


def dot(a, b):
    return lax.dot_general(a, b, (((1,), (0,)), ((), ())), preferred_element_type=F32)


def dot_t(a, b):
    return lax.dot_general(a, b, (((1,), (1,)), ((), ())), preferred_element_type=F32)


def iota(shape, dim):
    return lax.broadcasted_iota(jnp.int32, shape, dim)


def call(kernel, out_shape, specs, name):
    outs = jax.tree.map(lambda _: VMEM, out_shape)
    return pl.pallas_call(
        kernel,
        out_shape=out_shape,
        in_specs=specs,
        out_specs=outs,
        name=name,
        compiler_params=pltpu.CompilerParams(vmem_limit_bytes=48 * 1024 * 1024),
    )


def rms(values, gains):
    wide = values.astype(F32)
    scale = lax.rsqrt(jnp.mean(wide * wide, axis=-1, keepdims=True) + EPS)
    return (wide * scale) * gains.astype(F32)


def pack_kernel(core, wq, wo, routes, weights, out):
    start = core[0] * HALF
    ids = routes[...].astype(F32)
    wts = weights[...]
    high = wts.astype(BF16).astype(F32)
    low = wts - high
    lane = iota((OWN, 128), 1)
    info = jnp.zeros((OWN, 128), F32)
    for place, column in enumerate(
        (ids[:, 0:1], ids[:, 1:2], high[:, 0:1], low[:, 0:1], high[:, 1:2], low[:, 1:2])
    ):
        info = jnp.where(lane == place, column, info)
    info = jnp.concatenate([info, info], axis=0).astype(BF16)
    q_half = wq[pl.ds(pl.multiple_of(start, HALF), HALF), :]
    for d in range(TP):
        out[d, 0:HALF, :] = q_half
        out[d, 2 * HALF : 2 * HALF + 8, :] = info
    for j in range(4):
        block = wo[:, pl.ds(pl.multiple_of(start + j * 128, 128), 128)]
        for d in range(TP):
            out[d, HALF + 128 * j : HALF + 128 * (j + 1), :] = block


def norm_kernel(tokens, gain, wk, wv, attn_in, new_k, new_v):
    a = rms(tokens[...], gain[...]).astype(BF16)
    attn_in[...] = a
    new_k[...] = dot(a, wk[...]).astype(BF16)
    new_v[...] = dot(a, wv[...]).astype(BF16)


def expert_pack_kernel(gate, up, down, out):
    out[0:D, :] = gate[...]
    out[D : 2 * D, :] = up[...]
    for j in range(4):
        out[2 * D + 256 * j : 2 * D + 256 * (j + 1), :] = down[:, 256 * j : 256 * (j + 1)]


def attend_kernel(
    core, lengths, tokens, attn_in, w_own, w_sib, bias, keys, values, gain, residual, sent
):
    first = core[0] == 0

    def ordered(a, b):
        return jnp.where(first, a, b)

    a = attn_in[...].astype(F32)
    x_own = ordered(a[:, :HALF], a[:, HALF:]).astype(BF16)
    x_sib = ordered(a[:, HALF:], a[:, :HALF]).astype(BF16)
    q = jnp.concatenate(
        [dot(x_own, w_own[t, 0:HALF, :]) + dot(x_sib, w_sib[t, 0:HALF, :]) for t in range(TP)],
        axis=1,
    )
    q = q.astype(BF16).astype(F32)
    head_mask = iota((HEADS, HEADS * HEAD), 1) // HEAD == iota((HEADS, HEADS * HEAD), 0)
    spread = jnp.concatenate(
        [
            jnp.where(head_mask, jnp.broadcast_to(q[b : b + 1], (HEADS, HEADS * HEAD)), 0.0)
            for b in range(OWN)
        ],
        axis=0,
    ).astype(BF16)
    source = iota((HEADS * HEAD, 128), 0)
    fold = (
        (source // (HEADS * HEAD // KV)) * HEAD + source % HEAD == iota((HEADS * HEAD, 128), 1)
    ).astype(F32)
    fold = fold.astype(BF16)
    q_blocks = dot(spread, fold).astype(BF16)
    position = iota((HEADS, CACHE), 1)
    logs, skips, lives = [], [], []
    for b in range(OWN):
        s = dot_t(q_blocks[8 * b : 8 * b + 8], keys[b])
        s = s * (1.0 / math.sqrt(HEAD)) + bias[...]
        tail = jnp.log1p(jnp.exp(-jnp.abs(s)))
        live = position < lengths[b]
        logs.append(jnp.minimum(s, 0.0) - tail)
        skips.append(jnp.where(live, jnp.minimum(-s, 0.0) - tail, 0.0))
        lives.append(live)
    chunks = CACHE // 128
    stacked = jnp.concatenate(
        [skips[b][:, 128 * k : 128 * k + 128] for b in range(OWN) for k in range(chunks)], axis=0
    )
    after = (iota((128, 128), 0) > iota((128, 128), 1)).astype(F32).astype(BF16)
    p1 = stacked.astype(BF16)
    rest = stacked - p1.astype(F32)
    p2 = rest.astype(BF16)
    p3 = (rest - p2.astype(F32)).astype(BF16)
    inner = dot(p1, after) + dot(p2, after) + dot(p3, after)
    totals = jnp.sum(stacked, axis=1, keepdims=True)
    mixes = []
    for b in range(OWN):
        carry = jnp.zeros((HEADS, 1), F32)
        later = [None] * chunks
        for k in reversed(range(chunks)):
            row = 8 * (b * chunks + k)
            later[k] = inner[row : row + 8] + carry
            carry = carry + totals[row : row + 8]
        later = jnp.concatenate(later, axis=1)
        weights = jnp.where(lives[b], jnp.exp(logs[b] + later), 0.0).astype(BF16)
        mixes.append(dot(weights, values[b]))
    mixed = jnp.concatenate(mixes, axis=0).astype(BF16)
    wide = dot_t(mixed, fold)
    mixed = jnp.concatenate(
        [
            jnp.sum(jnp.where(head_mask, wide[8 * b : 8 * b + 8], 0.0), axis=0, keepdims=True)
            for b in range(OWN)
        ],
        axis=0,
    ).astype(BF16)

    def project(w):
        parts = []
        for j in range(4):
            row = HALF + 128 * j
            acc = dot(mixed[:, 0:128], w[0, row : row + 128, :])
            for t in range(1, TP):
                acc = acc + dot(mixed[:, 128 * t : 128 * t + 128], w[t, row : row + 128, :])
            parts.append(acc)
        return jnp.concatenate(parts, axis=1)

    out_own, out_sib = project(w_own), project(w_sib)
    total = jnp.concatenate([ordered(out_own, out_sib), ordered(out_sib, out_own)], axis=1)
    res = (tokens[...].astype(F32) + total).astype(BF16)
    residual[...] = res
    f = rms(res, gain[...])
    f = jnp.concatenate([f[:, :HALF], f[:, HALF:]], axis=0).astype(BF16)
    for d in range(TP):
        sent[d] = f


def dispatch_kernel(tp, group, info, mix_gate, sent, combine):
    n = TP * 8
    row, col = iota((n, ROWS), 0), iota((n, ROWS), 1)
    facts = info[...].astype(F32)
    id0, id1 = facts[:, 0:1], facts[:, 1:2]
    w0, w1 = facts[:, 2:3] + facts[:, 3:4], facts[:, 4:5] + facts[:, 5:6]
    chip, r = col // MSG, col % 4
    expert = (chip // 2).astype(F32)
    is0, is1 = id0 == expert, id1 == expert
    chosen = jnp.where(is0 | is1, 1.0, 0.0)
    ra, rb = iota((n, n), 0), iota((n, n), 1)
    before = ((rb // 4) % 2 == 0) & (rb // 8 * 4 + rb % 4 < ra // 8 * 4 + ra % 4)
    earlier = dot(before.astype(F32).astype(BF16), chosen.astype(BF16))
    same_half = (row // 4) % 2 == (col // 4) % 2
    slot = same_half & (r < 2) & (chosen > 0.5) & (earlier == r.astype(F32))
    mine = same_half & (r >= 2) & (row // 8 == tp[0]) & (row % 4 == r - 2 + 2 * (chip % 2))
    g = group[...]
    pick = jnp.where(slot | mine, 1.0, 0.0)
    sent[...] = dot(pick.T.astype(BF16), g).astype(BF16)
    first_half = (iota((n, 1), 0) // 4) % 2 == 0
    gates = mix_gate[...].astype(F32)
    gate_rows = jnp.where(first_half, gates[0:1, :], gates[1:2, :])
    part = jnp.sum(g.astype(F32) * gate_rows, axis=1, keepdims=True)
    part = jnp.broadcast_to(part, (n, 128))
    other = jnp.where(first_half, pltpu.roll(part, n - 4, 0), pltpu.roll(part, 4, 0))
    mix = 1.0 / (1.0 + jnp.exp(-(part + other)))
    weight = jnp.where(slot, jnp.where(is0, w0, w1), jnp.where(mine, mix[:, 0:1], 0.0))
    high = weight.astype(BF16)
    combine[0] = high
    combine[1] = (weight - high.astype(F32)).astype(BF16)


def expert_kernel(x, gate, up, down, sib, dense_a, dense_b, out):
    rows = CHIPS * 4
    i, k = iota((rows, ROWS), 0), iota((rows, ROWS), 1)
    at = (i // 4) * MSG + i % 4
    halves = [(k == at + 4 * h).astype(F32).astype(BF16) for h in range(2)]
    got = x[...]
    xs = jnp.concatenate([dot(p, got) for p in halves], axis=1).astype(BF16)
    is_slot = iota((rows, 1), 0) % 4 < 2

    def hidden(g, u, keep):
        return jnp.where(keep, g / (1.0 + jnp.exp(-g)) * u, 0.0).astype(BF16)

    h_own = hidden(dot(xs, gate[...]), dot(xs, up[...]), is_slot)
    h_sib = hidden(dot(xs, sib[0:D, :]), dot(xs, sib[D : 2 * D, :]), is_slot)
    blocks = (dense_a, 0), (dense_a, 96), (dense_b, 0), (dense_b, 96)

    def stack(base):
        return jnp.concatenate([ref[off + base : off + base + 32, :] for ref, off in blocks], axis=0)

    h_dense = hidden(dot_t(xs, stack(0)), dot_t(xs, stack(32)), jnp.logical_not(is_slot))
    total = dot(h_own, down[...]) + dot(h_dense, stack(64))
    total = total + jnp.concatenate(
        [dot(h_sib, sib[2 * D + 256 * j : 2 * D + 256 * (j + 1), :]) for j in range(4)], axis=1
    )
    total = total.astype(BF16)
    i, k = iota((ROWS, rows), 1), iota((ROWS, rows), 0)
    at = (i // 4) * MSG + i % 4
    res = None
    for h in range(2):
        p = (k == at + 4 * h).astype(F32).astype(BF16)
        part = dot(p, total[:, HALF * h : HALF * (h + 1)])
        res = part if res is None else res + part
    out[...] = res.astype(BF16)


def combine_kernel(combine, returned, out):
    got = returned[...]
    total = dot(combine[0], got) + dot(combine[1], got)
    out[...] = total.astype(BF16)


def finish_kernel(residual, parts, out):
    total = parts[0].astype(F32)
    for t in range(1, TP):
        total = total + parts[t].astype(F32)
    total = jnp.concatenate([total[0:4, :], total[4:8, :]], axis=1)
    out[...] = (residual[...].astype(F32) + total).astype(BF16)


def shape(*dims, dtype=BF16):
    return jax.ShapeDtypeStruct(dims, dtype)


def a2a(array, axis):
    return lax.all_to_all(array, axis, split_axis=0, concat_axis=0, tiled=True)


def swap(array, axis):
    return lax.ppermute(array, axis, [(i, i ^ 1) for i in range(lax.axis_size(axis))])


def body(
    tokens,
    gain_attn,
    gain_ffn,
    w_query,
    w_key,
    w_value,
    w_output,
    head_bias,
    keys_cache,
    values_cache,
    lengths,
    dense_gate_w,
    dense_up_w,
    dense_down_w,
    mix_gate,
    expert_gate,
    expert_up,
    expert_down,
    routes,
    route_weights,
):
    core = lax.axis_index("c").astype(jnp.int32).reshape(1)
    tp = lax.axis_index("x").astype(jnp.int32).reshape(1)
    wlen = 2 * HALF + 8
    packed = call(
        pack_kernel, shape(TP, wlen, 128), [SMEM, VMEM, VMEM, VMEM, VMEM], "pack_weights"
    )(core, w_query, w_output, routes, route_weights)
    w_own = a2a(packed, "x")
    w_sib = swap(w_own, "c")
    dense_own = jnp.concatenate([dense_gate_w, dense_up_w, dense_down_w], axis=0)
    dense_a = jnp.concatenate([dense_own, swap(dense_own, "c")], axis=0)
    dense_b = swap(dense_a, "y")
    expert_own = call(expert_pack_kernel, shape(3 * D, 256), [VMEM] * 3, "pack_experts")(
        expert_gate[0], expert_up[0], expert_down[0]
    )
    expert_sib = swap(expert_own, "c")
    attn_in, new_keys, new_values = call(
        norm_kernel,
        (shape(OWN, D), shape(OWN, 128), shape(OWN, 128)),
        [VMEM] * 4,
        "norm",
    )(tokens, gain_attn.reshape(1, D), w_key, w_value)
    residual, sent = call(
        attend_kernel,
        (shape(OWN, D), shape(TP, 8, HALF)),
        [SMEM, SMEM] + [VMEM] * 8,
        "attend",
    )(
        core,
        lengths,
        tokens,
        attn_in,
        w_own,
        w_sib,
        head_bias.reshape(HEADS, 1),
        keys_cache,
        values_cache,
        gain_ffn.reshape(1, D),
    )
    group = a2a(sent, "x").reshape(TP * 8, HALF)
    info = w_own[:, 2 * HALF :, :].reshape(TP * 8, 128)
    rows, combine = call(
        dispatch_kernel,
        (shape(ROWS, HALF), shape(2, TP * 8, ROWS)),
        [SMEM] + [VMEM] * 3,
        "dispatch",
    )(tp, group, info, mix_gate.reshape(2, HALF))
    received = a2a(rows.reshape(CHIPS, MSG, HALF), ("z", "y")).reshape(ROWS, HALF)
    outs = call(expert_kernel, shape(ROWS, HALF), [VMEM] * 7, "experts")(
        received, expert_gate[0], expert_up[0], expert_down[0], expert_sib, dense_a, dense_b
    )
    returned = a2a(outs.reshape(CHIPS, MSG, HALF), ("z", "y")).reshape(ROWS, HALF)
    partial = call(combine_kernel, shape(TP * 8, HALF), [VMEM] * 2, "combine")(combine, returned)
    parts = a2a(partial.reshape(TP, 8, HALF), "x")
    layer_out = call(finish_kernel, shape(OWN, D), [VMEM] * 2, "finish")(residual, parts)
    return (layer_out, new_keys, new_values)


def solution(mesh):
    grid = Mesh(mesh.devices.reshape(8, 8, 2, TP), ("z", "y", "c", "x"))
    ep = ("z", "y", "c")
    every = ("z", "y", "c", "x")
    return jax.shard_map(
        body,
        mesh=grid,
        in_specs=(
            P(every, None),
            P(),
            P(),
            P(None, "x"),
            P(),
            P(),
            P("x", None),
            P(),
            P(every, None, None),
            P(every, None, None),
            P(every),
            P(ep, None),
            P(ep, None),
            P(ep, None),
            P(),
            P(ep, None, "x"),
            P(ep, None, "x"),
            P(ep, "x", None),
            P(every, None),
            P(every, None),
        ),
        out_specs=(P(every, None), P(every, None), P(every, None)),
        check_vma=False,
    )
```

```python
import math

import jax
import jax.numpy as jnp
from jax import lax
from jax.experimental import pallas as pl
from jax.experimental.pallas import tpu as pltpu
from jax.sharding import Mesh, PartitionSpec as P


HEADS = 8
KV = 2
HEAD = 64
EPS = 1e-06
D = 1024
HALF = D // 2
CACHE = 1024
OWN = 4
TP = 4
CHIPS = 64
MSG = 8
ROWS = CHIPS * MSG
F32 = jnp.float32
BF16 = jnp.bfloat16


VMEM = pl.BlockSpec(memory_space=pltpu.VMEM)
SMEM = pl.BlockSpec(memory_space=pltpu.SMEM)
HBM = pl.BlockSpec(memory_space=pltpu.HBM)
EXPERT_ROWS = 3 * D
DENSE_ROWS = 96
SIB_SCRATCH = [
    pltpu.VMEM((EXPERT_ROWS + 8 * DENSE_ROWS, 256), jnp.bfloat16),
    pltpu.SemaphoreType.DMA((7,)),
]


def dot(a, b):
    return lax.dot_general(a, b, (((1,), (0,)), ((), ())), preferred_element_type=F32)


def dot_t(a, b):
    return lax.dot_general(a, b, (((1,), (1,)), ((), ())), preferred_element_type=F32)


def iota(shape, dim):
    return lax.broadcasted_iota(jnp.int32, shape, dim)


def call(kernel, out_shape, specs, scratch=(), limit=4):
    outs = jax.tree.map(lambda _: VMEM, out_shape)
    return pl.pallas_call(
        kernel,
        out_shape=out_shape,
        in_specs=specs,
        out_specs=outs,
        scratch_shapes=list(scratch),
        compiler_params=pltpu.CompilerParams(vmem_limit_bytes=limit * 1024 * 1024),
    )


def rms(values, gains):
    wide = values.astype(F32)
    scale = lax.rsqrt(jnp.mean(wide * wide, axis=-1, keepdims=True) + EPS)
    return (wide * scale) * gains.astype(F32)


def pack_kernel(core, wq, wo, routes_hbm, weights_hbm, gate, up, down, out, dense, routes, weights, sems):
    start = core[0] * HALF
    facts = [
        pltpu.make_async_copy(routes_hbm, routes, sems.at[8]),
        pltpu.make_async_copy(weights_hbm, weights, sems.at[9]),
    ]
    for c in facts:
        c.start()
    copies = [
        pltpu.make_async_copy(
            wq.at[pl.ds(pl.multiple_of(start, HALF), HALF), :], out.at[0, 0:HALF, :], sems.at[0]
        )
    ]
    for j in range(4):
        copies.append(
            pltpu.make_async_copy(
                wo.at[:, pl.ds(pl.multiple_of(start + j * 128, 128), 128)],
                out.at[0, HALF + 128 * j : HALF + 128 * (j + 1), :],
                sems.at[1 + j],
            )
        )
    for k, ref in enumerate((gate, up, down)):
        copies.append(
            pltpu.make_async_copy(ref, dense.at[32 * k : 32 * (k + 1), :], sems.at[5 + k])
        )
    for c in copies:
        c.start()
    for c in facts:
        c.wait()
    eye = iota((OWN, OWN), 0) == iota((OWN, OWN), 1)

    def column(row):
        return jnp.sum(jnp.where(eye, row, 0.0), axis=1, keepdims=True)

    ids, wts = routes[...].astype(F32), weights[...]
    high = wts.astype(BF16).astype(F32)
    low = wts - high
    lane = iota((OWN, 128), 1)
    info = jnp.zeros((OWN, 128), F32)
    for place, row in enumerate((ids[0:1], ids[1:2], high[0:1], low[0:1], high[1:2], low[1:2])):
        info = jnp.where(lane == place, column(row), info)
    info = jnp.concatenate([info, info], axis=0).astype(BF16)
    for d in range(TP):
        out[d, 2 * HALF : 2 * HALF + 8, :] = info
    for c in copies:
        c.wait()
    for d in range(1, TP):
        out[d, 0 : 2 * HALF, :] = out[0, 0 : 2 * HALF, :]


def norm_kernel(tokens, gain, wk, wv, attn_in, new_k, new_v):
    a = rms(tokens[...], gain[...]).astype(BF16)
    attn_in[...] = a
    new_k[...] = dot(a, wk[...]).astype(BF16)
    new_v[...] = dot(a, wv[...]).astype(BF16)


def expert_pack_kernel(gate, up, down, dense_own, dense_y, out):
    out[0:D, :] = gate[...]
    out[D : 2 * D, :] = up[...]
    base = 2 * D
    for ref in (down, dense_own, dense_y):
        n = ref.shape[0]
        for j in range(4):
            out[base : base + n, :] = ref[:, 256 * j : 256 * (j + 1)]
            base = base + n


def attend_kernel(
    core, lengths, tokens, attn_in, w_own, w_sib, bias, keys, values, gain, residual, sent
):
    first = core[0] == 0

    def ordered(a, b):
        return jnp.where(first, a, b)

    a = attn_in[...].astype(F32)
    x_own = ordered(a[:, :HALF], a[:, HALF:]).astype(BF16)
    x_sib = ordered(a[:, HALF:], a[:, :HALF]).astype(BF16)
    q = jnp.concatenate(
        [dot(x_own, w_own[t, 0:HALF, :]) + dot(x_sib, w_sib[t, 0:HALF, :]) for t in range(TP)],
        axis=1,
    )
    q = q.astype(BF16).astype(F32)
    head_mask = iota((HEADS, HEADS * HEAD), 1) // HEAD == iota((HEADS, HEADS * HEAD), 0)
    spread = jnp.concatenate(
        [
            jnp.where(head_mask, jnp.broadcast_to(q[b : b + 1], (HEADS, HEADS * HEAD)), 0.0)
            for b in range(OWN)
        ],
        axis=0,
    ).astype(BF16)
    source = iota((HEADS * HEAD, 128), 0)
    fold = (
        (source // (HEADS * HEAD // KV)) * HEAD + source % HEAD == iota((HEADS * HEAD, 128), 1)
    ).astype(F32)
    fold = fold.astype(BF16)
    q_blocks = dot(spread, fold).astype(BF16)
    position = iota((HEADS, CACHE), 1)
    eye = iota((HEADS, HEADS), 0) == iota((HEADS, HEADS), 1)
    offset = jnp.sum(jnp.where(eye, bias[...], 0.0), axis=1, keepdims=True)
    logs, skips, lives = [], [], []
    for b in range(OWN):
        s = dot_t(q_blocks[8 * b : 8 * b + 8], keys[b])
        s = s * (1.0 / math.sqrt(HEAD)) + offset
        tail = jnp.log1p(jnp.exp(-jnp.abs(s)))
        live = position < lengths[b]
        logs.append(jnp.minimum(s, 0.0) - tail)
        skips.append(jnp.where(live, jnp.minimum(-s, 0.0) - tail, 0.0))
        lives.append(live)
    chunks = CACHE // 128
    stacked = jnp.concatenate(
        [skips[b][:, 128 * k : 128 * k + 128] for b in range(OWN) for k in range(chunks)], axis=0
    )
    after = (iota((128, 128), 0) > iota((128, 128), 1)).astype(F32).astype(BF16)
    p1 = stacked.astype(BF16)
    rest = stacked - p1.astype(F32)
    p2 = rest.astype(BF16)
    p3 = (rest - p2.astype(F32)).astype(BF16)
    inner = dot(p1, after) + dot(p2, after) + dot(p3, after)
    totals = jnp.sum(stacked, axis=1, keepdims=True)
    mixes = []
    for b in range(OWN):
        carry = jnp.zeros((HEADS, 1), F32)
        later = [None] * chunks
        for k in reversed(range(chunks)):
            row = 8 * (b * chunks + k)
            later[k] = inner[row : row + 8] + carry
            carry = carry + totals[row : row + 8]
        later = jnp.concatenate(later, axis=1)
        weights = jnp.where(lives[b], jnp.exp(logs[b] + later), 0.0).astype(BF16)
        mixes.append(dot(weights, values[b]))
    mixed = jnp.concatenate(mixes, axis=0).astype(BF16)
    wide = dot_t(mixed, fold)
    mixed = jnp.concatenate(
        [
            jnp.sum(jnp.where(head_mask, wide[8 * b : 8 * b + 8], 0.0), axis=0, keepdims=True)
            for b in range(OWN)
        ],
        axis=0,
    ).astype(BF16)

    def project(w):
        parts = []
        for j in range(4):
            row = HALF + 128 * j
            acc = dot(mixed[:, 0:128], w[0, row : row + 128, :])
            for t in range(1, TP):
                acc = acc + dot(mixed[:, 128 * t : 128 * t + 128], w[t, row : row + 128, :])
            parts.append(acc)
        return jnp.concatenate(parts, axis=1)

    out_own, out_sib = project(w_own), project(w_sib)
    total = jnp.concatenate([ordered(out_own, out_sib), ordered(out_sib, out_own)], axis=1)
    res = (tokens[...].astype(F32) + total).astype(BF16)
    residual[...] = res
    f = rms(res, gain[...])
    f = jnp.concatenate([f[:, :HALF], f[:, HALF:]], axis=0).astype(BF16)
    for d in range(TP):
        sent[d] = f


def table_kernel(
    tp, own_hbm, keys_hbm, values_hbm, pick, weight, mine_out, own, keys, values, sems
):
    copies = [
        [pltpu.make_async_copy(src.at[b], dst.at[b], sems.at[k, b]) for b in range(OWN)]
        for k, (src, dst) in enumerate(((own_hbm, own), (keys_hbm, keys), (values_hbm, values)))
    ]
    for group in copies:
        for c in group:
            c.start()
    for c in copies[0]:
        c.wait()
    n = TP * 8
    row, col = iota((n, ROWS), 0), iota((n, ROWS), 1)
    facts = jnp.concatenate([own[t, 2 * HALF :, :] for t in range(TP)], axis=0).astype(F32)
    id0, id1 = facts[:, 0:1], facts[:, 1:2]
    w0, w1 = facts[:, 2:3] + facts[:, 3:4], facts[:, 4:5] + facts[:, 5:6]
    chip, r = col // MSG, col % 4
    expert = (chip // 2).astype(F32)
    is0, is1 = id0 == expert, id1 == expert
    chosen = jnp.where(is0 | is1, 1.0, 0.0)
    ra, rb = iota((n, n), 0), iota((n, n), 1)
    before = ((rb // 4) % 2 == 0) & (rb // 8 * 4 + rb % 4 < ra // 8 * 4 + ra % 4)
    earlier = dot(before.astype(F32).astype(BF16), chosen.astype(BF16))
    same_half = (row // 4) % 2 == (col // 4) % 2
    slot = same_half & (r < 2) & (chosen > 0.5) & (earlier == r.astype(F32))
    mine = same_half & (r >= 2) & (row // 8 == tp[0]) & (row % 4 == r - 2 + 2 * (chip % 2))
    pick[...] = jnp.where(slot | mine, 1.0, 0.0).T.astype(BF16)
    weight[...] = jnp.where(slot, jnp.where(is0, w0, w1), 0.0)
    mine_out[...] = jnp.where(mine, 1.0, 0.0)
    for group in copies[1:]:
        for c in group:
            c.wait()


def send_kernel(pick, group, sent):
    sent[...] = dot(pick[...], group[...]).astype(BF16)


def mix_kernel(group, mix_gate, mix):
    n = TP * 8
    first_half = (iota((n, 1), 0) // 4) % 2 == 0
    gates = mix_gate[...].astype(F32)
    gate_rows = jnp.where(first_half, gates[0:1, :], gates[1:2, :])
    part = jnp.sum(group[...].astype(F32) * gate_rows, axis=1, keepdims=True)
    part = jnp.broadcast_to(part, (n, 128))
    other = jnp.where(first_half, pltpu.roll(part, n - 4, 0), pltpu.roll(part, 4, 0))
    mix[...] = 1.0 / (1.0 + jnp.exp(-(part + other)))


def weigh_kernel(mix, weight, mine, combine):
    total = weight[...] + mine[...] * mix[:, 0:1]
    high = total.astype(BF16)
    combine[0] = high
    combine[1] = (total - high.astype(F32)).astype(BF16)


def expert_kernel(x, gate, up, down, sib_hbm, dense_own, dense_y, out, sib, sems):
    edges = [0, D // 2, D, 3 * D // 2, 2 * D, 5 * D // 2, EXPERT_ROWS, EXPERT_ROWS + 8 * DENSE_ROWS]
    copies = [
        pltpu.make_async_copy(sib_hbm.at[lo:hi, :], sib.at[lo:hi, :], sems.at[k])
        for k, (lo, hi) in enumerate(zip(edges[:-1], edges[1:]))
    ]
    for c in copies:
        c.start()
    rows = CHIPS * 4
    i, k = iota((rows, ROWS), 0), iota((rows, ROWS), 1)
    at = (i // 4) * MSG + i % 4
    halves = [(k == at + 4 * h).astype(F32).astype(BF16) for h in range(2)]
    got = x[...]
    xs = jnp.concatenate([dot(p, got) for p in halves], axis=1).astype(BF16)
    is_slot = iota((rows, 1), 0) % 4 < 2

    def hidden(g, u, keep):
        return jnp.where(keep, g / (1.0 + jnp.exp(-g)) * u, 0.0).astype(BF16)

    h_own = hidden(dot(xs, gate[...]), dot(xs, up[...]), is_slot)
    total = dot(h_own, down[...])
    for c in copies:
        c.wait()
    h_sib = hidden(dot(xs, sib[0:D, :]), dot(xs, sib[D : 2 * D, :]), is_slot)

    def stack(base):
        parts = [ref[base : base + 32, :] for ref in (dense_own, dense_y)]
        for k in range(2):
            first = EXPERT_ROWS + 4 * DENSE_ROWS * k + base
            parts.append(
                jnp.concatenate(
                    [sib[first + DENSE_ROWS * j : first + DENSE_ROWS * j + 32, :] for j in range(4)],
                    axis=1,
                )
            )
        return jnp.concatenate(parts, axis=0)

    h_dense = hidden(dot_t(xs, stack(0)), dot_t(xs, stack(32)), jnp.logical_not(is_slot))
    total = total + dot(h_dense, stack(64))
    total = total + jnp.concatenate(
        [dot(h_sib, sib[2 * D + 256 * j : 2 * D + 256 * (j + 1), :]) for j in range(4)], axis=1
    )
    total = total.astype(BF16)
    i, k = iota((ROWS, rows), 1), iota((ROWS, rows), 0)
    at = (i // 4) * MSG + i % 4
    res = None
    for h in range(2):
        p = (k == at + 4 * h).astype(F32).astype(BF16)
        part = dot(p, total[:, HALF * h : HALF * (h + 1)])
        res = part if res is None else res + part
    out[...] = res.astype(BF16)


def combine_kernel(combine, returned, out):
    got = returned[...]
    total = dot(combine[0], got) + dot(combine[1], got)
    out[...] = total.astype(BF16)


def finish_kernel(residual, parts, out):
    total = parts[0].astype(F32)
    for t in range(1, TP):
        total = total + parts[t].astype(F32)
    total = jnp.concatenate([total[0:4, :], total[4:8, :]], axis=1)
    out[...] = (residual[...].astype(F32) + total).astype(BF16)


def in_hbm(array):
    return pltpu.with_memory_space_constraint(array, pltpu.HBM)


def in_vmem(array):
    return pltpu.with_memory_space_constraint(array, pltpu.VMEM)


def shape(*dims, dtype=BF16):
    return jax.ShapeDtypeStruct(dims, dtype)


def a2a(array, axis):
    return lax.all_to_all(array, axis, split_axis=0, concat_axis=0, tiled=True)


def swap(array, axis):
    return lax.ppermute(array, axis, [(i, i ^ 1) for i in range(lax.axis_size(axis))])


def body(
    tokens,
    gain_attn,
    gain_ffn,
    w_query,
    w_key,
    w_value,
    w_output,
    head_bias,
    keys_cache,
    values_cache,
    lengths,
    dense_gate_w,
    dense_up_w,
    dense_down_w,
    mix_gate,
    expert_gate,
    expert_up,
    expert_down,
    routes,
    route_weights,
):
    core = lax.axis_index("c").astype(jnp.int32).reshape(1)
    tp = lax.axis_index("x").astype(jnp.int32).reshape(1)
    wlen = 2 * HALF + 8
    packed, dense_own = call(
        pack_kernel,
        (shape(TP, wlen, 128), shape(DENSE_ROWS, D)),
        [SMEM] + [HBM] * 7,
        [pltpu.VMEM((2, OWN), jnp.int32), pltpu.VMEM((2, OWN), F32), pltpu.SemaphoreType.DMA((10,))],
    )(
        core,
        in_hbm(w_query),
        in_hbm(w_output),
        in_hbm(routes.T),
        in_hbm(route_weights.T),
        in_hbm(dense_gate_w),
        in_hbm(dense_up_w),
        in_hbm(dense_down_w),
    )
    w_own = a2a(packed, "x")
    w_sib = swap(w_own, "c")
    dense_y = swap(dense_own, "y")
    expert_own = call(
        expert_pack_kernel, shape(EXPERT_ROWS + 8 * DENSE_ROWS, 256), [VMEM] * 5, limit=8
    )(expert_gate[0], expert_up[0], expert_down[0], dense_own, dense_y)
    expert_sib = swap(expert_own, "c")
    attn_in, new_keys, new_values = call(
        norm_kernel, (shape(OWN, D), shape(OWN, 128), shape(OWN, 128)), [VMEM] * 4
    )(tokens, gain_attn.reshape(1, D), w_key, w_value)
    cache = pltpu.VMEM((OWN, CACHE, 128), BF16)
    pick, weight, mine, w_here, keys, values = call(
        table_kernel,
        (
            shape(ROWS, TP * 8),
            shape(TP * 8, ROWS, dtype=F32),
            shape(TP * 8, ROWS, dtype=F32),
            pltpu.VMEM((TP, wlen, 128), BF16),
            cache,
            cache,
        ),
        [SMEM, HBM, HBM, HBM],
        [pltpu.SemaphoreType.DMA((3, OWN))],
    )(tp, in_hbm(w_own), in_hbm(keys_cache), in_hbm(values_cache))
    residual, sent = call(
        attend_kernel, (shape(OWN, D), shape(TP, 8, HALF)), [SMEM, SMEM] + [VMEM] * 8
    )(
        core,
        lengths,
        tokens,
        attn_in,
        in_vmem(w_here),
        in_vmem(w_sib),
        head_bias.reshape(1, HEADS),
        in_vmem(keys),
        in_vmem(values),
        gain_ffn.reshape(1, D),
    )
    group = a2a(sent, "x")
    group = group.reshape(TP * 8, HALF)
    rows = call(send_kernel, shape(ROWS, HALF), [VMEM] * 2)(pick, group)
    mix = call(mix_kernel, shape(TP * 8, 128, dtype=F32), [VMEM] * 2)(
        group, mix_gate.reshape(2, HALF)
    )
    combine = call(weigh_kernel, shape(2, TP * 8, ROWS), [VMEM] * 3)(
        mix, weight, mine
    )
    received = a2a(rows.reshape(CHIPS, MSG, HALF), ("z", "y"))
    outs = call(expert_kernel, shape(ROWS, HALF), [VMEM] * 4 + [HBM] + [VMEM] * 2, SIB_SCRATCH, 16)(
        received.reshape(ROWS, HALF),
        expert_gate[0],
        expert_up[0],
        expert_down[0],
        in_hbm(expert_sib),
        dense_own,
        dense_y,
    )
    returned = a2a(outs.reshape(CHIPS, MSG, HALF), ("z", "y"))
    partial = call(combine_kernel, shape(TP * 8, HALF), [VMEM] * 2)(
        combine, returned.reshape(ROWS, HALF)
    )
    parts = a2a(partial.reshape(TP, 8, HALF), "x")
    layer_out = call(finish_kernel, shape(OWN, D), [VMEM] * 2)(residual, parts)
    return (layer_out, new_keys, new_values)


def solution(mesh):
    grid = Mesh(mesh.devices.reshape(8, 8, 2, TP), ("z", "y", "c", "x"))
    ep = ("z", "y", "c")
    every = ("z", "y", "c", "x")
    return jax.shard_map(
        body,
        mesh=grid,
        in_specs=(
            P(every, None),
            P(),
            P(),
            P(None, "x"),
            P(),
            P(),
            P("x", None),
            P(),
            P(every, None, None),
            P(every, None, None),
            P(every),
            P(ep, None),
            P(ep, None),
            P(ep, None),
            P(),
            P(ep, None, "x"),
            P(ep, None, "x"),
            P(ep, "x", None),
            P(every, None),
            P(every, None),
        ),
        out_specs=(P(every, None), P(every, None), P(every, None)),
        check_vma=False,
    )
```

```python
import math

import jax
import jax.numpy as jnp
from jax import lax
from jax.experimental import pallas as pl
from jax.experimental.pallas import tpu as pltpu
from jax.sharding import Mesh, PartitionSpec as P


HEADS = 8
KV = 2
HEAD = 64
EPS = 1e-06
D = 1024
HALF = D // 2
CACHE = 1024
OWN = 4
TP = 4
CHIPS = 64
MSG = 8
ROWS = CHIPS * MSG
F32 = jnp.float32
BF16 = jnp.bfloat16


VMEM = pl.BlockSpec(memory_space=pltpu.VMEM)
SMEM = pl.BlockSpec(memory_space=pltpu.SMEM)
HBM = pl.BlockSpec(memory_space=pltpu.HBM)
EXPERT_ROWS = 3 * D
DENSE_ROWS = 96
PACK = EXPERT_ROWS + 4 * DENSE_ROWS


def dot(a, b):
    return lax.dot_general(a, b, (((1,), (0,)), ((), ())), preferred_element_type=F32)


def dot_t(a, b):
    return lax.dot_general(a, b, (((1,), (1,)), ((), ())), preferred_element_type=F32)


def iota(shape, dim):
    return lax.broadcasted_iota(jnp.int32, shape, dim)


def call(kernel, out_shape, specs, scratch=(), limit=4, outs=VMEM):
    outs = jax.tree.map(lambda _: outs, out_shape)
    return pl.pallas_call(
        kernel,
        out_shape=out_shape,
        in_specs=specs,
        out_specs=outs,
        scratch_shapes=list(scratch),
        compiler_params=pltpu.CompilerParams(vmem_limit_bytes=limit * 1024 * 1024),
    )


def rms(values, gains):
    wide = values.astype(F32)
    scale = lax.rsqrt(jnp.mean(wide * wide, axis=-1, keepdims=True) + EPS)
    return (wide * scale) * gains.astype(F32)


def pack_kernel(
    core, wq, wo, routes_hbm, weights_hbm, gate, up, down, out, dense, routes, weights, half, rows, sems
):
    start = core[0] * HALF
    facts = [
        pltpu.make_async_copy(routes_hbm, routes, sems.at[0]),
        pltpu.make_async_copy(weights_hbm, weights, sems.at[1]),
    ]
    reads = [(wq.at[pl.ds(pl.multiple_of(start, HALF), HALF), :], half.at[0:HALF, :])]
    for j in range(4):
        block = wo.at[:, pl.ds(pl.multiple_of(start + j * 128, 128), 128)]
        reads.append((block, half.at[HALF + 128 * j : HALF + 128 * (j + 1), :]))
    reads = [pltpu.make_async_copy(a, b, sems.at[2 + k]) for k, (a, b) in enumerate(reads)]
    shared = [
        pltpu.make_async_copy(ref, rows.at[32 * k : 32 * (k + 1), :], sems.at[7 + k])
        for k, ref in enumerate((gate, up, down))
    ]
    for c in facts + reads + shared:
        c.start()
    for c in facts:
        c.wait()
    eye = iota((OWN, OWN), 0) == iota((OWN, OWN), 1)

    def column(row):
        return jnp.sum(jnp.where(eye, row, 0.0), axis=1, keepdims=True)

    ids, wts = routes[...].astype(F32), weights[...]
    high = wts.astype(BF16).astype(F32)
    low = wts - high
    lane = iota((OWN, 128), 1)
    info = jnp.zeros((OWN, 128), F32)
    for place, row in enumerate((ids[0:1], ids[1:2], high[0:1], low[0:1], high[1:2], low[1:2])):
        info = jnp.where(lane == place, column(row), info)
    half[2 * HALF : 2 * HALF + 8, :] = jnp.concatenate([info, info], axis=0).astype(BF16)
    for c in reads:
        c.wait()
    sends = [pltpu.make_async_copy(half, out.at[d], sems.at[10 + d]) for d in range(TP)]
    for c in sends:
        c.start()
    for c in shared:
        c.wait()
    last = pltpu.make_async_copy(rows, dense, sems.at[14])
    last.start()
    for c in sends:
        c.wait()
    last.wait()


def norm_kernel(tokens, gain, attn_in):
    attn_in[...] = rms(tokens[...], gain[...]).astype(BF16)


def kv_kernel(attn_in, wk, wv, new_k, new_v):
    a = attn_in[...]
    new_k[...] = dot(a, wk[...]).astype(BF16)
    new_v[...] = dot(a, wv[...]).astype(BF16)


def expert_pack_kernel(gate, up, down, dense, out, here, sems):
    reads = [
        (ref.at[h * HALF : (h + 1) * HALF, :], D * k + HALF * h, HALF)
        for k, ref in enumerate((gate, up))
        for h in range(2)
    ]
    base = 2 * D
    for ref in (down, dense):
        n = ref.shape[0]
        for j in range(4):
            reads.append((ref.at[:, 256 * j : 256 * (j + 1)], base, n))
            base = base + n
    ins, outs = [], []
    for k, (src, first, n) in enumerate(reads):
        place = here.at[first : first + n, :]
        ins.append(pltpu.make_async_copy(src, place, sems.at[0, k]))
        outs.append(pltpu.make_async_copy(place, out.at[first : first + n, :], sems.at[1, k]))
    for c in ins:
        c.start()
    for a, b in zip(ins, outs):
        a.wait()
        b.start()
    for c in outs:
        c.wait()


def fetch_kernel(*refs):
    n = (len(refs) - 1) // 2
    sems = refs[-1]
    copies = []
    for k in range(n):
        rows = refs[k].shape[0]
        step = rows // 4
        for q in range(4):
            part = slice(q * step, (q + 1) * step)
            copies.append(
                pltpu.make_async_copy(
                    refs[k].at[part, :], refs[n + k].at[part, :], sems.at[k, q]
                )
            )
    for c in copies:
        c.start()
    for c in copies:
        c.wait()


def attend_kernel(
    core, lengths, tokens, attn_in, w_own, w_sib, bias, keys, values, gain, residual, sent
):
    first = core[0] == 0

    def ordered(a, b):
        return jnp.where(first, a, b)

    a = attn_in[...].astype(F32)
    x_own = ordered(a[:, :HALF], a[:, HALF:]).astype(BF16)
    x_sib = ordered(a[:, HALF:], a[:, :HALF]).astype(BF16)
    q = jnp.concatenate(
        [dot(x_own, w_own[t, 0:HALF, :]) + dot(x_sib, w_sib[t, 0:HALF, :]) for t in range(TP)],
        axis=1,
    )
    q = q.astype(BF16).astype(F32)
    head_mask = iota((HEADS, HEADS * HEAD), 1) // HEAD == iota((HEADS, HEADS * HEAD), 0)
    spread = jnp.concatenate(
        [
            jnp.where(head_mask, jnp.broadcast_to(q[b : b + 1], (HEADS, HEADS * HEAD)), 0.0)
            for b in range(OWN)
        ],
        axis=0,
    ).astype(BF16)
    source = iota((HEADS * HEAD, 128), 0)
    fold = (
        (source // (HEADS * HEAD // KV)) * HEAD + source % HEAD == iota((HEADS * HEAD, 128), 1)
    ).astype(F32)
    fold = fold.astype(BF16)
    q_blocks = dot(spread, fold).astype(BF16)
    position = iota((HEADS, CACHE), 1)
    eye = iota((HEADS, HEADS), 0) == iota((HEADS, HEADS), 1)
    offset = jnp.sum(jnp.where(eye, bias[...], 0.0), axis=1, keepdims=True)
    logs, skips, lives = [], [], []
    for b in range(OWN):
        s = dot_t(q_blocks[8 * b : 8 * b + 8], keys[b])
        s = s * (1.0 / math.sqrt(HEAD)) + offset
        tail = jnp.log1p(jnp.exp(-jnp.abs(s)))
        live = position < lengths[b]
        logs.append(jnp.minimum(s, 0.0) - tail)
        skips.append(jnp.where(live, jnp.minimum(-s, 0.0) - tail, 0.0))
        lives.append(live)
    chunks = CACHE // 128
    stacked = jnp.concatenate(
        [skips[b][:, 128 * k : 128 * k + 128] for b in range(OWN) for k in range(chunks)], axis=0
    )
    after = (iota((128, 128), 0) > iota((128, 128), 1)).astype(F32).astype(BF16)
    p1 = stacked.astype(BF16)
    rest = stacked - p1.astype(F32)
    p2 = rest.astype(BF16)
    p3 = (rest - p2.astype(F32)).astype(BF16)
    inner = dot(p1, after) + dot(p2, after) + dot(p3, after)
    totals = jnp.sum(stacked, axis=1, keepdims=True)
    mixes = []
    for b in range(OWN):
        carry = jnp.zeros((HEADS, 1), F32)
        later = [None] * chunks
        for k in reversed(range(chunks)):
            row = 8 * (b * chunks + k)
            later[k] = inner[row : row + 8] + carry
            carry = carry + totals[row : row + 8]
        later = jnp.concatenate(later, axis=1)
        weights = jnp.where(lives[b], jnp.exp(logs[b] + later), 0.0).astype(BF16)
        mixes.append(dot(weights, values[b]))
    mixed = jnp.concatenate(mixes, axis=0).astype(BF16)
    wide = dot_t(mixed, fold)
    mixed = jnp.concatenate(
        [
            jnp.sum(jnp.where(head_mask, wide[8 * b : 8 * b + 8], 0.0), axis=0, keepdims=True)
            for b in range(OWN)
        ],
        axis=0,
    ).astype(BF16)

    def project(w):
        parts = []
        for j in range(4):
            row = HALF + 128 * j
            acc = dot(mixed[:, 0:128], w[0, row : row + 128, :])
            for t in range(1, TP):
                acc = acc + dot(mixed[:, 128 * t : 128 * t + 128], w[t, row : row + 128, :])
            parts.append(acc)
        return jnp.concatenate(parts, axis=1)

    out_own, out_sib = project(w_own), project(w_sib)
    total = jnp.concatenate([ordered(out_own, out_sib), ordered(out_sib, out_own)], axis=1)
    res = (tokens[...].astype(F32) + total).astype(BF16)
    residual[...] = res
    f = rms(res, gain[...])
    f = jnp.concatenate([f[:, :HALF], f[:, HALF:]], axis=0).astype(BF16)
    for d in range(TP):
        sent[d] = f


def table_kernel(
    tp, own_hbm, keys_hbm, values_hbm, pick, weight, mine_out, own, keys, values, sems
):
    copies = [
        [pltpu.make_async_copy(src.at[b], dst.at[b], sems.at[k, b]) for b in range(OWN)]
        for k, (src, dst) in enumerate(((own_hbm, own), (keys_hbm, keys), (values_hbm, values)))
    ]
    for group in copies:
        for c in group:
            c.start()
    for c in copies[0]:
        c.wait()
    n = TP * 8
    row, col = iota((n, ROWS), 0), iota((n, ROWS), 1)
    facts = jnp.concatenate([own[t, 2 * HALF :, :] for t in range(TP)], axis=0).astype(F32)
    id0, id1 = facts[:, 0:1], facts[:, 1:2]
    w0, w1 = facts[:, 2:3] + facts[:, 3:4], facts[:, 4:5] + facts[:, 5:6]
    chip, r = col // MSG, col % 4
    expert = (chip // 2).astype(F32)
    is0, is1 = id0 == expert, id1 == expert
    chosen = jnp.where(is0 | is1, 1.0, 0.0)
    ra, rb = iota((n, n), 0), iota((n, n), 1)
    before = ((rb // 4) % 2 == 0) & (rb // 8 * 4 + rb % 4 < ra // 8 * 4 + ra % 4)
    earlier = dot(before.astype(F32).astype(BF16), chosen.astype(BF16))
    same_half = (row // 4) % 2 == (col // 4) % 2
    slot = same_half & (r < 2) & (chosen > 0.5) & (earlier == r.astype(F32))
    mine = same_half & (r >= 2) & (row // 8 == tp[0]) & (row % 4 == r - 2 + 2 * (chip % 2))
    pick[...] = jnp.where(slot | mine, 1.0, 0.0).T.astype(BF16)
    weight[...] = jnp.where(slot, jnp.where(is0, w0, w1), 0.0)
    mine_out[...] = jnp.where(mine, 1.0, 0.0)
    for group in copies[1:]:
        for c in group:
            c.wait()


def send_kernel(pick, group, out, here, sems):
    for b in range(ROWS // 256):
        part = dot(pick[256 * b : 256 * (b + 1), :], group[...])
        send_rows(part, here, out, 256 * b, sems.at[b])
    for b in range(ROWS // 256):
        send_wait(here, out, 256 * b, sems.at[b])


def mix_kernel(group, mix_gate, mix):
    n = TP * 8
    first_half = (iota((n, 1), 0) // 4) % 2 == 0
    gates = mix_gate[...].astype(F32)
    gate_rows = jnp.where(first_half, gates[0:1, :], gates[1:2, :])
    part = jnp.sum(group[...].astype(F32) * gate_rows, axis=1, keepdims=True)
    part = jnp.broadcast_to(part, (n, 128))
    other = jnp.where(first_half, pltpu.roll(part, n - 4, 0), pltpu.roll(part, 4, 0))
    mix[...] = 1.0 / (1.0 + jnp.exp(-(part + other)))


def weigh_kernel(mix, weight, mine, combine):
    total = weight[...] + mine[...] * mix[:, 0:1]
    high = total.astype(BF16)
    combine[0] = high
    combine[1] = (total - high.astype(F32)).astype(BF16)


def rows_copy(here, out, first, sem):
    part = slice(first, first + 256)
    return pltpu.make_async_copy(here.at[part, :], out.at[part, :], sem)


def send_rows(values, here, out, first, sem):
    here[first : first + 256, :] = values.astype(BF16)
    rows_copy(here, out, first, sem).start()


def send_wait(here, out, first, sem):
    rows_copy(here, out, first, sem).wait()


def expert_kernel(x, own_hbm, sib, dense_y, dense_yc, out, own, here, sems):
    step = PACK // 8
    copies = [
        pltpu.make_async_copy(
            own_hbm.at[k * step : (k + 1) * step, :], own.at[k * step : (k + 1) * step, :], sems.at[k]
        )
        for k in range(8)
    ]
    for c in copies:
        c.start()

    def place(dim):
        k = iota((256, 256), dim)
        i = k % 64
        return (i // 2) * MSG + i % 2 + 2 * (k // 64 % 2) + 4 * (k // 128)

    order = (iota((256, 256), 1) == place(0)).astype(F32).astype(BF16)
    back = (iota((256, 256), 0) == place(1)).astype(F32).astype(BF16)
    blocks = ROWS // 256
    xs, xd = [], []
    for b in range(blocks):
        y = dot(order, x[256 * b : 256 * (b + 1), :]).astype(BF16)
        xs.append(jnp.concatenate([y[0:64], y[128:192]], axis=1))
        xd.append(jnp.concatenate([y[64:128], y[192:256]], axis=1))
    xs, xd = jnp.concatenate(xs, axis=0), jnp.concatenate(xd, axis=0)

    def hidden(g, u):
        return (g / (1.0 + jnp.exp(-g)) * u).astype(BF16)

    total = None
    for w in (sib, own):
        if w is own:
            for c in copies:
                c.wait()
        h = hidden(dot(xs, w[0:D, :]), dot(xs, w[D : 2 * D, :]))
        part = jnp.concatenate(
            [dot(h, w[2 * D + 256 * j : 2 * D + 256 * (j + 1), :]) for j in range(4)], axis=1
        )
        total = part if total is None else total + part

    def stack(base):
        parts = [ref[base : base + 32, :] for ref in (dense_y, dense_yc)]
        for w in (own, sib):
            first = EXPERT_ROWS + base
            parts.append(
                jnp.concatenate(
                    [w[first + DENSE_ROWS * j : first + DENSE_ROWS * j + 32, :] for j in range(4)],
                    axis=1,
                )
            )
        return jnp.concatenate(parts, axis=0)

    h_dense = hidden(dot_t(xd, stack(0)), dot_t(xd, stack(32)))
    dense = dot(h_dense, stack(64)).astype(BF16)
    total = total.astype(BF16)
    for b in range(blocks):
        part = jnp.concatenate([total[64 * b : 64 * (b + 1)], dense[64 * b : 64 * (b + 1)]], axis=0)
        part = jnp.concatenate([part[:, :HALF], part[:, HALF:]], axis=0)
        send_rows(dot(back, part), here, out, 256 * b, sems.at[8 + b])
    for b in range(blocks):
        send_wait(here, out, 256 * b, sems.at[8 + b])


def combine_kernel(combine, returned, out):
    got = returned[...]
    total = dot(combine[0], got) + dot(combine[1], got)
    out[...] = total.astype(BF16)


def finish_kernel(residual, parts, out):
    total = parts[0].astype(F32)
    for t in range(1, TP):
        total = total + parts[t].astype(F32)
    total = jnp.concatenate([total[0:4, :], total[4:8, :]], axis=1)
    out[...] = (residual[...].astype(F32) + total).astype(BF16)


def in_hbm(array):
    return pltpu.with_memory_space_constraint(array, pltpu.HBM)


def in_vmem(array):
    return pltpu.with_memory_space_constraint(array, pltpu.VMEM)


def shape(*dims, dtype=BF16):
    return jax.ShapeDtypeStruct(dims, dtype)


def a2a(array, axis):
    return lax.all_to_all(array, axis, split_axis=0, concat_axis=0, tiled=True)


def swap(array, axis):
    return lax.ppermute(array, axis, [(i, i ^ 1) for i in range(lax.axis_size(axis))])


def body(
    tokens,
    gain_attn,
    gain_ffn,
    w_query,
    w_key,
    w_value,
    w_output,
    head_bias,
    keys_cache,
    values_cache,
    lengths,
    dense_gate_w,
    dense_up_w,
    dense_down_w,
    mix_gate,
    expert_gate,
    expert_up,
    expert_down,
    routes,
    route_weights,
):
    core = lax.axis_index("c").astype(jnp.int32).reshape(1)
    tp = lax.axis_index("x").astype(jnp.int32).reshape(1)
    wlen = 2 * HALF + 8
    packed, dense_own = call(
        pack_kernel,
        (pltpu.HBM((TP, wlen, 128), BF16), pltpu.HBM((DENSE_ROWS, D), BF16)),
        [SMEM] + [HBM] * 7,
        [
            pltpu.VMEM((2, OWN), jnp.int32),
            pltpu.VMEM((2, OWN), F32),
            pltpu.VMEM((wlen, 128), BF16),
            pltpu.VMEM((DENSE_ROWS, D), BF16),
            pltpu.SemaphoreType.DMA((15,)),
        ],
        outs=HBM,
    )(
        core,
        in_hbm(w_query),
        in_hbm(w_output),
        in_hbm(routes.T),
        in_hbm(route_weights.T),
        in_hbm(dense_gate_w),
        in_hbm(dense_up_w),
        in_hbm(dense_down_w),
    )
    w_own = a2a(packed, "x")
    w_sib = swap(w_own, "c")
    dense_y = swap(dense_own, "y")
    expert_own = call(
        expert_pack_kernel,
        pltpu.HBM((PACK, 256), BF16),
        [HBM] * 4,
        [pltpu.VMEM((PACK, 256), BF16), pltpu.SemaphoreType.DMA((2, 12))],
        outs=HBM,
    )(
        in_hbm(expert_gate[0]),
        in_hbm(expert_up[0]),
        in_hbm(expert_down[0]),
        in_hbm(dense_own),
    )
    expert_sib = swap(expert_own, "c")
    dense_yc = swap(dense_y, "c")
    attn_in = call(norm_kernel, shape(OWN, D), [VMEM] * 2)(tokens, gain_attn.reshape(1, D))
    new_keys, new_values = call(
        kv_kernel, (shape(OWN, 128), shape(OWN, 128)), [VMEM] * 3
    )(attn_in, w_key, w_value)
    cache = pltpu.VMEM((OWN, CACHE, 128), BF16)
    pick, weight, mine, w_here, keys, values = call(
        table_kernel,
        (
            shape(ROWS, TP * 8),
            shape(TP * 8, ROWS, dtype=F32),
            shape(TP * 8, ROWS, dtype=F32),
            pltpu.VMEM((TP, wlen, 128), BF16),
            cache,
            cache,
        ),
        [SMEM, HBM, HBM, HBM],
        [pltpu.SemaphoreType.DMA((3, OWN))],
    )(tp, in_hbm(w_own), in_hbm(keys_cache), in_hbm(values_cache))
    residual, sent = call(
        attend_kernel, (shape(OWN, D), shape(TP, 8, HALF)), [SMEM, SMEM] + [VMEM] * 8
    )(
        core,
        lengths,
        tokens,
        attn_in,
        in_vmem(w_here),
        in_vmem(w_sib),
        head_bias.reshape(1, HEADS),
        in_vmem(keys),
        in_vmem(values),
        gain_ffn.reshape(1, D),
    )
    group = a2a(sent, "x")
    group = group.reshape(TP * 8, HALF)
    rows = call(
        send_kernel,
        pltpu.HBM((ROWS, HALF), BF16),
        [VMEM] * 2,
        [pltpu.VMEM((ROWS, HALF), BF16), pltpu.SemaphoreType.DMA((2,))],
        outs=HBM,
    )(pick, group)
    mix = call(mix_kernel, shape(TP * 8, 128, dtype=F32), [VMEM] * 2)(
        group, mix_gate.reshape(2, HALF)
    )
    combine = call(weigh_kernel, shape(2, TP * 8, ROWS), [VMEM] * 3)(
        mix, weight, mine
    )
    received = a2a(rows.reshape(CHIPS, MSG, HALF), ("z", "y"))
    sources = (expert_sib, dense_y, dense_yc)
    fetched = call(
        fetch_kernel,
        tuple(pltpu.VMEM(a.shape, BF16) for a in sources),
        [HBM] * 3,
        [pltpu.SemaphoreType.DMA((3, 4))],
        8,
    )(*(in_hbm(a) for a in sources))
    outs = call(
        expert_kernel,
        pltpu.HBM((ROWS, HALF), BF16),
        [VMEM, HBM] + [VMEM] * 3,
        [
            pltpu.VMEM((PACK, 256), BF16),
            pltpu.VMEM((ROWS, HALF), BF16),
            pltpu.SemaphoreType.DMA((10,)),
        ],
        16,
        HBM,
    )(received.reshape(ROWS, HALF), in_hbm(expert_own), *(in_vmem(a) for a in fetched))
    returned = a2a(outs.reshape(CHIPS, MSG, HALF), ("z", "y"))
    partial = call(combine_kernel, shape(TP * 8, HALF), [VMEM] * 2)(
        combine, returned.reshape(ROWS, HALF)
    )
    parts = a2a(partial.reshape(TP, 8, HALF), "x")
    layer_out = call(finish_kernel, shape(OWN, D), [VMEM] * 2)(residual, parts)
    return (layer_out, new_keys, new_values)


def solution(mesh):
    grid = Mesh(mesh.devices.reshape(8, 8, 2, TP), ("z", "y", "c", "x"))
    ep = ("z", "y", "c")
    every = ("z", "y", "c", "x")
    return jax.shard_map(
        body,
        mesh=grid,
        in_specs=(
            P(every, None),
            P(),
            P(),
            P(None, "x"),
            P(),
            P(),
            P("x", None),
            P(),
            P(every, None, None),
            P(every, None, None),
            P(every),
            P(ep, None),
            P(ep, None),
            P(ep, None),
            P(),
            P(ep, None, "x"),
            P(ep, None, "x"),
            P(ep, "x", None),
            P(every, None),
            P(every, None),
        ),
        out_specs=(P(every, None), P(every, None), P(every, None)),
        check_vma=False,
    )
```

```python
import math

import jax
import jax.numpy as jnp
from jax import lax
from jax.experimental import pallas as pl
from jax.experimental.pallas import tpu as pltpu
from jax.sharding import Mesh, PartitionSpec as P


HEADS = 8
KV = 2
HEAD = 64
EPS = 1e-06
D = 1024
HALF = D // 2
CACHE = 1024
OWN = 4
TP = 4
CHIPS = 64
MSG = 8
ROWS = CHIPS * MSG
F32 = jnp.float32
BF16 = jnp.bfloat16


VMEM = pl.BlockSpec(memory_space=pltpu.VMEM)
SMEM = pl.BlockSpec(memory_space=pltpu.SMEM)
HBM = pl.BlockSpec(memory_space=pltpu.HBM)
EXPERT_ROWS = 3 * D
DENSE_ROWS = 96
PACK = EXPERT_ROWS + 4 * DENSE_ROWS


def dot(a, b):
    return lax.dot_general(a, b, (((1,), (0,)), ((), ())), preferred_element_type=F32)


def dot_t(a, b):
    return lax.dot_general(a, b, (((1,), (1,)), ((), ())), preferred_element_type=F32)


def iota(shape, dim):
    return lax.broadcasted_iota(jnp.int32, shape, dim)


def call(kernel, out_shape, specs, scratch=(), limit=4, outs=VMEM):
    outs = jax.tree.map(lambda _: outs, out_shape)
    return pl.pallas_call(
        kernel,
        out_shape=out_shape,
        in_specs=specs,
        out_specs=outs,
        scratch_shapes=list(scratch),
        compiler_params=pltpu.CompilerParams(vmem_limit_bytes=limit * 1024 * 1024),
    )


def rms(values, gains):
    wide = values.astype(F32)
    scale = lax.rsqrt(jnp.mean(wide * wide, axis=-1, keepdims=True) + EPS)
    return (wide * scale) * gains.astype(F32)


def pack_kernel(
    core, wq, wo, routes_hbm, weights_hbm, gate, up, down, out, dense, routes, weights, half, rows, sems
):
    start = core[0] * HALF
    facts = [
        pltpu.make_async_copy(routes_hbm, routes, sems.at[0]),
        pltpu.make_async_copy(weights_hbm, weights, sems.at[1]),
    ]
    reads = [(wq.at[pl.ds(pl.multiple_of(start, HALF), HALF), :], half.at[0:HALF, :])]
    for j in range(4):
        block = wo.at[:, pl.ds(pl.multiple_of(start + j * 128, 128), 128)]
        reads.append((block, half.at[HALF + 128 * j : HALF + 128 * (j + 1), :]))
    reads = [pltpu.make_async_copy(a, b, sems.at[2 + k]) for k, (a, b) in enumerate(reads)]
    shared = [
        pltpu.make_async_copy(ref, rows.at[32 * k : 32 * (k + 1), :], sems.at[7 + k])
        for k, ref in enumerate((gate, up, down))
    ]
    for c in facts + reads + shared:
        c.start()
    for c in facts:
        c.wait()
    eye = iota((OWN, OWN), 0) == iota((OWN, OWN), 1)

    def column(row):
        return jnp.sum(jnp.where(eye, row, 0.0), axis=1, keepdims=True)

    ids, wts = routes[...].astype(F32), weights[...]
    high = wts.astype(BF16).astype(F32)
    low = wts - high
    lane = iota((OWN, 128), 1)
    info = jnp.zeros((OWN, 128), F32)
    for place, row in enumerate((ids[0:1], ids[1:2], high[0:1], low[0:1], high[1:2], low[1:2])):
        info = jnp.where(lane == place, column(row), info)
    half[2 * HALF : 2 * HALF + 8, :] = jnp.concatenate([info, info], axis=0).astype(BF16)
    for c in reads:
        c.wait()
    sends = [pltpu.make_async_copy(half, out.at[d], sems.at[10 + d]) for d in range(TP)]
    for c in sends:
        c.start()
    for c in shared:
        c.wait()
    last = pltpu.make_async_copy(rows, dense, sems.at[14])
    last.start()
    for c in sends:
        c.wait()
    last.wait()


def norm_kernel(tokens, gain, attn_in):
    attn_in[...] = rms(tokens[...], gain[...]).astype(BF16)


def kv_kernel(attn_in, wk, wv, new_k, new_v):
    a = attn_in[...]
    new_k[...] = dot(a, wk[...]).astype(BF16)
    new_v[...] = dot(a, wv[...]).astype(BF16)


def expert_pack_kernel(gate, up, down, dense, out, here, sems):
    reads = [
        (ref.at[h * HALF : (h + 1) * HALF, :], D * k + HALF * h, HALF)
        for k, ref in enumerate((gate, up))
        for h in range(2)
    ]
    base = 2 * D
    for ref in (down, dense):
        n = ref.shape[0]
        for j in range(4):
            reads.append((ref.at[:, 256 * j : 256 * (j + 1)], base, n))
            base = base + n
    ins, outs = [], []
    for k, (src, first, n) in enumerate(reads):
        place = here.at[first : first + n, :]
        ins.append(pltpu.make_async_copy(src, place, sems.at[0, k]))
        outs.append(pltpu.make_async_copy(place, out.at[first : first + n, :], sems.at[1, k]))
    for c in ins:
        c.start()
    for a, b in zip(ins, outs):
        a.wait()
        b.start()
    for c in outs:
        c.wait()


def fetch_kernel(*refs):
    n = (len(refs) - 1) // 2
    sems = refs[-1]
    copies = []
    for k in range(n):
        rows = refs[k].shape[0]
        step = rows // 4
        for q in range(4):
            part = slice(q * step, (q + 1) * step)
            copies.append(
                pltpu.make_async_copy(
                    refs[k].at[part, :], refs[n + k].at[part, :], sems.at[k, q]
                )
            )
    for c in copies:
        c.start()
    for c in copies:
        c.wait()


def attend_kernel(
    core, lengths, tokens, attn_in, w_own, w_sib, bias, keys, values, gain, residual, sent
):
    first = core[0] == 0

    def ordered(a, b):
        return jnp.where(first, a, b)

    a = attn_in[...].astype(F32)
    x_own = ordered(a[:, :HALF], a[:, HALF:]).astype(BF16)
    x_sib = ordered(a[:, HALF:], a[:, :HALF]).astype(BF16)
    q = sum(
        dot(a, jnp.concatenate([w[t, 0:HALF, :] for t in range(TP)], axis=1))
        for a, w in ((x_own, w_own), (x_sib, w_sib))
    )
    q = q.astype(BF16).astype(F32)
    head_mask = iota((HEADS, HEADS * HEAD), 1) // HEAD == iota((HEADS, HEADS * HEAD), 0)
    spread = jnp.concatenate(
        [
            jnp.where(head_mask, jnp.broadcast_to(q[b : b + 1], (HEADS, HEADS * HEAD)), 0.0)
            for b in range(OWN)
        ],
        axis=0,
    ).astype(BF16)
    source = iota((HEADS * HEAD, 128), 0)
    fold = (
        (source // (HEADS * HEAD // KV)) * HEAD + source % HEAD == iota((HEADS * HEAD, 128), 1)
    ).astype(F32)
    fold = fold.astype(BF16)
    q_blocks = dot(spread, fold).astype(BF16)
    position = iota((HEADS, CACHE), 1)
    eye = iota((HEADS, HEADS), 0) == iota((HEADS, HEADS), 1)
    offset = jnp.sum(jnp.where(eye, bias[...], 0.0), axis=1, keepdims=True)
    logs, skips, lives = [], [], []
    for b in range(OWN):
        s = dot_t(q_blocks[8 * b : 8 * b + 8], keys[b])
        s = s * (1.0 / math.sqrt(HEAD)) + offset
        tail = jnp.log1p(jnp.exp(-jnp.abs(s)))
        live = position < lengths[b]
        logs.append(jnp.minimum(s, 0.0) - tail)
        skips.append(jnp.where(live, jnp.minimum(-s, 0.0) - tail, 0.0))
        lives.append(live)
    chunks = CACHE // 128
    stacked = jnp.concatenate(
        [skips[b][:, 128 * k : 128 * k + 128] for b in range(OWN) for k in range(chunks)], axis=0
    )
    after = (iota((128, 128), 0) > iota((128, 128), 1)).astype(F32).astype(BF16)
    p1 = stacked.astype(BF16)
    rest = stacked - p1.astype(F32)
    p2 = rest.astype(BF16)
    p3 = (rest - p2.astype(F32)).astype(BF16)
    inner = dot(p1, after) + dot(p2, after) + dot(p3, after)
    totals = jnp.sum(stacked, axis=1, keepdims=True)
    mixes = []
    for b in range(OWN):
        carry = jnp.zeros((HEADS, 1), F32)
        later = [None] * chunks
        for k in reversed(range(chunks)):
            row = 8 * (b * chunks + k)
            later[k] = inner[row : row + 8] + carry
            carry = carry + totals[row : row + 8]
        later = jnp.concatenate(later, axis=1)
        weights = jnp.where(lives[b], jnp.exp(logs[b] + later), 0.0).astype(BF16)
        mixes.append(dot(weights, values[b]))
    mixed = jnp.concatenate(mixes, axis=0).astype(BF16)
    wide = dot_t(mixed, fold)
    mixed = jnp.concatenate(
        [
            jnp.sum(jnp.where(head_mask, wide[8 * b : 8 * b + 8], 0.0), axis=0, keepdims=True)
            for b in range(OWN)
        ],
        axis=0,
    ).astype(BF16)

    def project(w):
        rows = [
            jnp.concatenate([w[t, HALF + 128 * j : HALF + 128 * (j + 1), :] for j in range(4)], axis=1)
            for t in range(TP)
        ]
        return dot(mixed, jnp.concatenate(rows, axis=0))

    out_own, out_sib = project(w_own), project(w_sib)
    total = jnp.concatenate([ordered(out_own, out_sib), ordered(out_sib, out_own)], axis=1)
    res = (tokens[...].astype(F32) + total).astype(BF16)
    residual[...] = res
    f = rms(res, gain[...])
    f = jnp.concatenate([f[:, :HALF], f[:, HALF:]], axis=0).astype(BF16)
    for d in range(TP):
        sent[d] = f


def table_kernel(
    tp, own_hbm, keys_hbm, values_hbm, pick, weight, mine_out, own, keys, values, sems
):
    copies = [
        [pltpu.make_async_copy(src.at[b], dst.at[b], sems.at[k, b]) for b in range(OWN)]
        for k, (src, dst) in enumerate(((own_hbm, own), (keys_hbm, keys), (values_hbm, values)))
    ]
    for group in copies:
        for c in group:
            c.start()
    for c in copies[0]:
        c.wait()
    n = TP * 8
    row, col = iota((n, ROWS), 0), iota((n, ROWS), 1)
    facts = jnp.concatenate([own[t, 2 * HALF :, :] for t in range(TP)], axis=0).astype(F32)
    id0, id1 = facts[:, 0:1], facts[:, 1:2]
    w0, w1 = facts[:, 2:3] + facts[:, 3:4], facts[:, 4:5] + facts[:, 5:6]
    chip, r = col // MSG, col % 4
    expert = (chip // 2).astype(F32)
    is0, is1 = id0 == expert, id1 == expert
    chosen = jnp.where(is0 | is1, 1.0, 0.0)
    ra, rb = iota((n, n), 0), iota((n, n), 1)
    before = ((rb // 4) % 2 == 0) & (rb // 8 * 4 + rb % 4 < ra // 8 * 4 + ra % 4)
    earlier = dot(before.astype(F32).astype(BF16), chosen.astype(BF16))
    same_half = (row // 4) % 2 == (col // 4) % 2
    slot = same_half & (r < 2) & (chosen > 0.5) & (earlier == r.astype(F32))
    mine = same_half & (r >= 2) & (row // 8 == tp[0]) & (row % 4 == r - 2 + 2 * (chip % 2))
    pick[...] = jnp.where(slot | mine, 1.0, 0.0).T.astype(BF16)
    weight[...] = jnp.where(slot, jnp.where(is0, w0, w1), 0.0)
    mine_out[...] = jnp.where(mine, 1.0, 0.0)
    for group in copies[1:]:
        for c in group:
            c.wait()


def send_kernel(pick, group, out, here, sems):
    for b in range(ROWS // 256):
        part = dot(pick[256 * b : 256 * (b + 1), :], group[...])
        send_rows(part, here, out, 256 * b, sems.at[b])
    for b in range(ROWS // 256):
        send_wait(here, out, 256 * b, sems.at[b])


def mix_kernel(group, mix_gate, mix):
    n = TP * 8
    first_half = (iota((n, 1), 0) // 4) % 2 == 0
    gates = mix_gate[...].astype(F32)
    gate_rows = jnp.where(first_half, gates[0:1, :], gates[1:2, :])
    part = jnp.sum(group[...].astype(F32) * gate_rows, axis=1, keepdims=True)
    part = jnp.broadcast_to(part, (n, 128))
    other = jnp.where(first_half, pltpu.roll(part, n - 4, 0), pltpu.roll(part, 4, 0))
    mix[...] = 1.0 / (1.0 + jnp.exp(-(part + other)))


def weigh_kernel(mix, weight, mine, combine):
    total = weight[...] + mine[...] * mix[:, 0:1]
    high = total.astype(BF16)
    combine[0] = high
    combine[1] = (total - high.astype(F32)).astype(BF16)


def rows_copy(here, out, first, sem):
    part = slice(first, first + 256)
    return pltpu.make_async_copy(here.at[part, :], out.at[part, :], sem)


def send_rows(values, here, out, first, sem):
    here[first : first + 256, :] = values.astype(BF16)
    rows_copy(here, out, first, sem).start()


def send_wait(here, out, first, sem):
    rows_copy(here, out, first, sem).wait()


def expert_kernel(x, own_hbm, sib, dense_y, dense_yc, out, own, here, sems):
    step = PACK // 8
    copies = [
        pltpu.make_async_copy(
            own_hbm.at[k * step : (k + 1) * step, :], own.at[k * step : (k + 1) * step, :], sems.at[k]
        )
        for k in range(8)
    ]
    for c in copies:
        c.start()

    def place(dim):
        k = iota((256, 256), dim)
        i = k % 64
        return (i // 2) * MSG + i % 2 + 2 * (k // 64 % 2) + 4 * (k // 128)

    order = (iota((256, 256), 1) == place(0)).astype(F32).astype(BF16)
    back = (iota((256, 256), 0) == place(1)).astype(F32).astype(BF16)
    blocks = ROWS // 256
    xs, xd = [], []
    for b in range(blocks):
        y = dot(order, x[256 * b : 256 * (b + 1), :]).astype(BF16)
        xs.append(jnp.concatenate([y[0:64], y[128:192]], axis=1))
        xd.append(jnp.concatenate([y[64:128], y[192:256]], axis=1))
    xs, xd = jnp.concatenate(xs, axis=0), jnp.concatenate(xd, axis=0)

    def hidden(g, u):
        return (g / (1.0 + jnp.exp(-g)) * u).astype(BF16)

    total = None
    for w in (sib, own):
        if w is own:
            for c in copies:
                c.wait()
        h = hidden(dot(xs, w[0:D, :]), dot(xs, w[D : 2 * D, :]))
        part = jnp.concatenate(
            [dot(h, w[2 * D + 256 * j : 2 * D + 256 * (j + 1), :]) for j in range(4)], axis=1
        )
        total = part if total is None else total + part

    def stack(base):
        parts = [ref[base : base + 32, :] for ref in (dense_y, dense_yc)]
        for w in (own, sib):
            first = EXPERT_ROWS + base
            parts.append(
                jnp.concatenate(
                    [w[first + DENSE_ROWS * j : first + DENSE_ROWS * j + 32, :] for j in range(4)],
                    axis=1,
                )
            )
        return jnp.concatenate(parts, axis=0)

    h_dense = hidden(dot_t(xd, stack(0)), dot_t(xd, stack(32)))
    dense = dot(h_dense, stack(64)).astype(BF16)
    total = total.astype(BF16)
    for b in range(blocks):
        part = jnp.concatenate([total[64 * b : 64 * (b + 1)], dense[64 * b : 64 * (b + 1)]], axis=0)
        part = jnp.concatenate([part[:, :HALF], part[:, HALF:]], axis=0)
        send_rows(dot(back, part), here, out, 256 * b, sems.at[8 + b])
    for b in range(blocks):
        send_wait(here, out, 256 * b, sems.at[8 + b])


def combine_kernel(combine, returned, out):
    got = returned[...]
    total = dot(combine[0], got) + dot(combine[1], got)
    out[...] = total.astype(BF16)


def finish_kernel(residual, parts, out):
    total = parts[0].astype(F32)
    for t in range(1, TP):
        total = total + parts[t].astype(F32)
    total = jnp.concatenate([total[0:4, :], total[4:8, :]], axis=1)
    out[...] = (residual[...].astype(F32) + total).astype(BF16)


def in_hbm(array):
    return pltpu.with_memory_space_constraint(array, pltpu.HBM)


def in_vmem(array):
    return pltpu.with_memory_space_constraint(array, pltpu.VMEM)


def shape(*dims, dtype=BF16):
    return jax.ShapeDtypeStruct(dims, dtype)


def a2a(array, axis):
    return lax.all_to_all(array, axis, split_axis=0, concat_axis=0, tiled=True)


def swap(array, axis):
    return lax.ppermute(array, axis, [(i, i ^ 1) for i in range(lax.axis_size(axis))])


def body(
    tokens,
    gain_attn,
    gain_ffn,
    w_query,
    w_key,
    w_value,
    w_output,
    head_bias,
    keys_cache,
    values_cache,
    lengths,
    dense_gate_w,
    dense_up_w,
    dense_down_w,
    mix_gate,
    expert_gate,
    expert_up,
    expert_down,
    routes,
    route_weights,
):
    core = lax.axis_index("c").astype(jnp.int32).reshape(1)
    tp = lax.axis_index("x").astype(jnp.int32).reshape(1)
    wlen = 2 * HALF + 8
    packed, dense_own = call(
        pack_kernel,
        (pltpu.HBM((TP, wlen, 128), BF16), pltpu.HBM((DENSE_ROWS, D), BF16)),
        [SMEM] + [HBM] * 7,
        [
            pltpu.VMEM((2, OWN), jnp.int32),
            pltpu.VMEM((2, OWN), F32),
            pltpu.VMEM((wlen, 128), BF16),
            pltpu.VMEM((DENSE_ROWS, D), BF16),
            pltpu.SemaphoreType.DMA((15,)),
        ],
        outs=HBM,
    )(
        core,
        in_hbm(w_query),
        in_hbm(w_output),
        in_hbm(routes.T),
        in_hbm(route_weights.T),
        in_hbm(dense_gate_w),
        in_hbm(dense_up_w),
        in_hbm(dense_down_w),
    )
    w_own = a2a(packed, "x")
    w_sib = swap(w_own, "c")
    dense_y = swap(dense_own, "y")
    expert_own = call(
        expert_pack_kernel,
        pltpu.HBM((PACK, 256), BF16),
        [HBM] * 4,
        [pltpu.VMEM((PACK, 256), BF16), pltpu.SemaphoreType.DMA((2, 12))],
        outs=HBM,
    )(
        in_hbm(expert_gate[0]),
        in_hbm(expert_up[0]),
        in_hbm(expert_down[0]),
        in_hbm(dense_own),
    )
    expert_sib = swap(expert_own, "c")
    dense_yc = swap(dense_y, "c")
    attn_in = call(norm_kernel, shape(OWN, D), [VMEM] * 2)(tokens, gain_attn.reshape(1, D))
    new_keys, new_values = call(
        kv_kernel, (shape(OWN, 128), shape(OWN, 128)), [VMEM] * 3
    )(attn_in, w_key, w_value)
    cache = pltpu.VMEM((OWN, CACHE, 128), BF16)
    pick, weight, mine, w_here, keys, values = call(
        table_kernel,
        (
            shape(ROWS, TP * 8),
            shape(TP * 8, ROWS, dtype=F32),
            shape(TP * 8, ROWS, dtype=F32),
            pltpu.VMEM((TP, wlen, 128), BF16),
            cache,
            cache,
        ),
        [SMEM, HBM, HBM, HBM],
        [pltpu.SemaphoreType.DMA((3, OWN))],
    )(tp, in_hbm(w_own), in_hbm(keys_cache), in_hbm(values_cache))
    residual, sent = call(
        attend_kernel, (shape(OWN, D), shape(TP, 8, HALF)), [SMEM, SMEM] + [VMEM] * 8
    )(
        core,
        lengths,
        tokens,
        attn_in,
        in_vmem(w_here),
        in_vmem(w_sib),
        head_bias.reshape(1, HEADS),
        in_vmem(keys),
        in_vmem(values),
        gain_ffn.reshape(1, D),
    )
    group = a2a(sent, "x")
    group = group.reshape(TP * 8, HALF)
    rows = call(
        send_kernel,
        pltpu.HBM((ROWS, HALF), BF16),
        [VMEM] * 2,
        [pltpu.VMEM((ROWS, HALF), BF16), pltpu.SemaphoreType.DMA((2,))],
        outs=HBM,
    )(pick, group)
    mix = call(mix_kernel, shape(TP * 8, 128, dtype=F32), [VMEM] * 2)(
        group, mix_gate.reshape(2, HALF)
    )
    combine = call(weigh_kernel, shape(2, TP * 8, ROWS), [VMEM] * 3)(
        mix, weight, mine
    )
    received = a2a(rows.reshape(CHIPS, MSG, HALF), ("z", "y"))
    sources = (expert_sib, dense_y, dense_yc)
    fetched = call(
        fetch_kernel,
        tuple(pltpu.VMEM(a.shape, BF16) for a in sources),
        [HBM] * 3,
        [pltpu.SemaphoreType.DMA((3, 4))],
        8,
    )(*(in_hbm(a) for a in sources))
    outs = call(
        expert_kernel,
        pltpu.HBM((ROWS, HALF), BF16),
        [VMEM, HBM] + [VMEM] * 3,
        [
            pltpu.VMEM((PACK, 256), BF16),
            pltpu.VMEM((ROWS, HALF), BF16),
            pltpu.SemaphoreType.DMA((10,)),
        ],
        16,
        HBM,
    )(received.reshape(ROWS, HALF), in_hbm(expert_own), *(in_vmem(a) for a in fetched))
    returned = a2a(outs.reshape(CHIPS, MSG, HALF), ("z", "y"))
    partial = call(combine_kernel, shape(TP * 8, HALF), [VMEM] * 2)(
        combine, returned.reshape(ROWS, HALF)
    )
    parts = a2a(partial.reshape(TP, 8, HALF), "x")
    layer_out = call(finish_kernel, shape(OWN, D), [VMEM] * 2)(residual, parts)
    return (layer_out, new_keys, new_values)


def solution(mesh):
    grid = Mesh(mesh.devices.reshape(8, 8, 2, TP), ("z", "y", "c", "x"))
    ep = ("z", "y", "c")
    every = ("z", "y", "c", "x")
    return jax.shard_map(
        body,
        mesh=grid,
        in_specs=(
            P(every, None),
            P(),
            P(),
            P(None, "x"),
            P(),
            P(),
            P("x", None),
            P(),
            P(every, None, None),
            P(every, None, None),
            P(every),
            P(ep, None),
            P(ep, None),
            P(ep, None),
            P(),
            P(ep, None, "x"),
            P(ep, None, "x"),
            P(ep, "x", None),
            P(every, None),
            P(every, None),
        ),
        out_specs=(P(every, None), P(every, None), P(every, None)),
        check_vma=False,
    )
```

```python
import math

import jax
import jax.numpy as jnp
from jax import lax
from jax.experimental import pallas as pl
from jax.experimental.pallas import tpu as pltpu
from jax.sharding import Mesh, PartitionSpec as P


HEADS = 8
KV = 2
HEAD = 64
EPS = 1e-06
D = 1024
HALF = D // 2
CACHE = 1024
OWN = 4
TP = 4
CHIPS = 64
MSG = 8
BLK = 8
SLOTS = 3
WIDE = SLOTS * 128
TOK = TP * BLK * 4
ROWS = CHIPS * MSG
F32 = jnp.float32
BF16 = jnp.bfloat16


VMEM = pl.BlockSpec(memory_space=pltpu.VMEM)
SMEM = pl.BlockSpec(memory_space=pltpu.SMEM)
HBM = pl.BlockSpec(memory_space=pltpu.HBM)
EXPERT_ROWS = 3 * D
DENSE_ROWS = 96
PACK = EXPERT_ROWS + 4 * DENSE_ROWS


def dot(a, b):
    return lax.dot_general(a, b, (((1,), (0,)), ((), ())), preferred_element_type=F32)


def dot_t(a, b):
    return lax.dot_general(a, b, (((1,), (1,)), ((), ())), preferred_element_type=F32)


def iota(shape, dim):
    return lax.broadcasted_iota(jnp.int32, shape, dim)


def call(kernel, out_shape, specs, scratch=(), limit=4, outs=VMEM):
    outs = jax.tree.map(lambda _: outs, out_shape)
    return pl.pallas_call(
        kernel,
        out_shape=out_shape,
        in_specs=specs,
        out_specs=outs,
        scratch_shapes=list(scratch),
        compiler_params=pltpu.CompilerParams(vmem_limit_bytes=limit * 1024 * 1024),
    )


def rms(values, gains):
    wide = values.astype(F32)
    scale = lax.rsqrt(jnp.mean(wide * wide, axis=-1, keepdims=True) + EPS)
    return (wide * scale) * gains.astype(F32)


def pack_kernel(
    core, wq, wo, routes_hbm, weights_hbm, gate, up, down, out, dense, routes, weights, half, rows, sems
):
    start = core[0] * HALF
    facts = [
        pltpu.make_async_copy(routes_hbm, routes, sems.at[0]),
        pltpu.make_async_copy(weights_hbm, weights, sems.at[1]),
    ]
    reads = [(wq.at[pl.ds(pl.multiple_of(start, HALF), HALF), :], half.at[0:HALF, :])]
    for j in range(4):
        block = wo.at[:, pl.ds(pl.multiple_of(start + j * 128, 128), 128)]
        reads.append((block, half.at[HALF + 128 * j : HALF + 128 * (j + 1), :]))
    reads = [pltpu.make_async_copy(a, b, sems.at[2 + k]) for k, (a, b) in enumerate(reads)]
    shared = [
        pltpu.make_async_copy(ref, rows.at[32 * k : 32 * (k + 1), :], sems.at[7 + k])
        for k, ref in enumerate((gate, up, down))
    ]
    for c in facts + reads + shared:
        c.start()
    for c in facts:
        c.wait()
    eye = iota((OWN, OWN), 0) == iota((OWN, OWN), 1)

    def column(row):
        return jnp.sum(jnp.where(eye, row, 0.0), axis=1, keepdims=True)

    ids, wts = routes[...].astype(F32), weights[...]
    high = wts.astype(BF16).astype(F32)
    low = wts - high
    lane = iota((OWN, 128), 1)
    info = jnp.zeros((OWN, 128), F32)
    for place, row in enumerate((ids[0:1], ids[1:2], high[0:1], low[0:1], high[1:2], low[1:2])):
        info = jnp.where(lane == place, column(row), info)
    half[2 * HALF : 2 * HALF + 8, :] = jnp.concatenate([info, info], axis=0).astype(BF16)
    for c in reads:
        c.wait()
    sends = [pltpu.make_async_copy(half, out.at[d], sems.at[10 + d]) for d in range(TP)]
    for c in sends:
        c.start()
    for c in shared:
        c.wait()
    last = pltpu.make_async_copy(rows, dense, sems.at[14])
    last.start()
    for c in sends:
        c.wait()
    last.wait()


def norm_kernel(tokens, gain, attn_in):
    attn_in[...] = rms(tokens[...], gain[...]).astype(BF16)


def kv_kernel(attn_in, wk, wv, new_k, new_v):
    a = attn_in[...]
    new_k[...] = dot(a, wk[...]).astype(BF16)
    new_v[...] = dot(a, wv[...]).astype(BF16)


def expert_pack_kernel(gate, up, down, dense, out, here, sems):
    reads = [
        (ref.at[h * HALF : (h + 1) * HALF, :], D * k + HALF * h, HALF)
        for k, ref in enumerate((gate, up))
        for h in range(2)
    ]
    base = 2 * D
    for ref in (down, dense):
        n = ref.shape[0]
        for j in range(4):
            reads.append((ref.at[:, 256 * j : 256 * (j + 1)], base, n))
            base = base + n
    ins, outs = [], []
    for k, (src, first, n) in enumerate(reads):
        place = here.at[first : first + n, :]
        ins.append(pltpu.make_async_copy(src, place, sems.at[0, k]))
        outs.append(pltpu.make_async_copy(place, out.at[first : first + n, :], sems.at[1, k]))
    for c in ins:
        c.start()
    for a, b in zip(ins, outs):
        a.wait()
        b.start()
    for c in outs:
        c.wait()


def join_kernel(a, b, c, out):
    for n, ref in enumerate((a, b, c)):
        out[DENSE_ROWS * n : DENSE_ROWS * (n + 1), :] = ref[...]


def fetch_kernel(*refs):
    n = (len(refs) - 1) // 2
    sems = refs[-1]
    copies = []
    for k in range(n):
        rows = refs[k].shape[0]
        step = rows // 4
        for q in range(4):
            part = slice(q * step, (q + 1) * step)
            copies.append(
                pltpu.make_async_copy(
                    refs[k].at[part, :], refs[n + k].at[part, :], sems.at[k, q]
                )
            )
    for c in copies:
        c.start()
    for c in copies:
        c.wait()


def attend_kernel(
    core, lengths, tokens, attn_in, w_own, w_sib, bias, keys, values, gain, residual, sent
):
    first = core[0] == 0

    def ordered(a, b):
        return jnp.where(first, a, b)

    a = attn_in[...].astype(F32)
    x_own = ordered(a[:, :HALF], a[:, HALF:]).astype(BF16)
    x_sib = ordered(a[:, HALF:], a[:, :HALF]).astype(BF16)
    q = sum(
        dot(a, jnp.concatenate([w[t, 0:HALF, :] for t in range(TP)], axis=1))
        for a, w in ((x_own, w_own), (x_sib, w_sib))
    )
    q = q.astype(BF16).astype(F32)
    head_mask = iota((HEADS, HEADS * HEAD), 1) // HEAD == iota((HEADS, HEADS * HEAD), 0)
    spread = jnp.concatenate(
        [
            jnp.where(head_mask, jnp.broadcast_to(q[b : b + 1], (HEADS, HEADS * HEAD)), 0.0)
            for b in range(OWN)
        ],
        axis=0,
    ).astype(BF16)
    source = iota((HEADS * HEAD, 128), 0)
    fold = (
        (source // (HEADS * HEAD // KV)) * HEAD + source % HEAD == iota((HEADS * HEAD, 128), 1)
    ).astype(F32)
    fold = fold.astype(BF16)
    q_blocks = dot(spread, fold).astype(BF16)
    position = iota((HEADS, CACHE), 1)
    eye = iota((HEADS, HEADS), 0) == iota((HEADS, HEADS), 1)
    offset = jnp.sum(jnp.where(eye, bias[...], 0.0), axis=1, keepdims=True)
    logs, skips, lives = [], [], []
    for b in range(OWN):
        s = dot_t(q_blocks[8 * b : 8 * b + 8], keys[b])
        s = s * (1.0 / math.sqrt(HEAD)) + offset
        tail = jnp.log1p(jnp.exp(-jnp.abs(s)))
        live = position < lengths[b]
        logs.append(jnp.minimum(s, 0.0) - tail)
        skips.append(jnp.where(live, jnp.minimum(-s, 0.0) - tail, 0.0))
        lives.append(live)
    chunks = CACHE // 128
    stacked = jnp.concatenate(
        [skips[b][:, 128 * k : 128 * k + 128] for b in range(OWN) for k in range(chunks)], axis=0
    )
    after = (iota((128, 128), 0) > iota((128, 128), 1)).astype(F32).astype(BF16)
    p1 = stacked.astype(BF16)
    rest = stacked - p1.astype(F32)
    p2 = rest.astype(BF16)
    p3 = (rest - p2.astype(F32)).astype(BF16)
    inner = dot(p1, after) + dot(p2, after) + dot(p3, after)
    totals = jnp.sum(stacked, axis=1, keepdims=True)
    mixes = []
    for b in range(OWN):
        carry = jnp.zeros((HEADS, 1), F32)
        later = [None] * chunks
        for k in reversed(range(chunks)):
            row = 8 * (b * chunks + k)
            later[k] = inner[row : row + 8] + carry
            carry = carry + totals[row : row + 8]
        later = jnp.concatenate(later, axis=1)
        weights = jnp.where(lives[b], jnp.exp(logs[b] + later), 0.0).astype(BF16)
        mixes.append(dot(weights, values[b]))
    mixed = jnp.concatenate(mixes, axis=0).astype(BF16)
    wide = dot_t(mixed, fold)
    mixed = jnp.concatenate(
        [
            jnp.sum(jnp.where(head_mask, wide[8 * b : 8 * b + 8], 0.0), axis=0, keepdims=True)
            for b in range(OWN)
        ],
        axis=0,
    ).astype(BF16)

    def project(w):
        rows = [
            jnp.concatenate([w[t, HALF + 128 * j : HALF + 128 * (j + 1), :] for j in range(4)], axis=1)
            for t in range(TP)
        ]
        return dot(mixed, jnp.concatenate(rows, axis=0))

    out_own, out_sib = project(w_own), project(w_sib)
    total = jnp.concatenate([ordered(out_own, out_sib), ordered(out_sib, out_own)], axis=1)
    res = (tokens[...].astype(F32) + total).astype(BF16)
    residual[...] = res
    f = rms(res, gain[...])
    f = jnp.concatenate([f[:, 128 * k : 128 * (k + 1)] for k in range(BLK)], axis=0).astype(BF16)
    for d in range(TP):
        sent[d] = f


def parts_of(token, place):
    same = (token // 4) % BLK == place % BLK
    chip = place // BLK
    return same, chip, token // 32, token % 4


def is_mine(tp, same, chip, t, i):
    return same & (t == tp) & (i == 2 * ((chip // 8) % 2) + chip % 2)


def before(first, second):
    return (
        ((first // 4) % BLK == 0) & (first // 32 * 4 + first % 4 < second // 32 * 4 + second % 4)
    ).astype(F32).astype(BF16)


def table_kernel(tp, own_hbm, keys_hbm, values_hbm, pick, info, own, keys, values, sems):
    copies = [
        [pltpu.make_async_copy(src.at[b], dst.at[b], sems.at[k, b]) for b in range(OWN)]
        for k, (src, dst) in enumerate(((own_hbm, own), (keys_hbm, keys), (values_hbm, values)))
    ]
    for group in copies:
        for c in group:
            c.start()
    for c in copies[0]:
        c.wait()
    facts = jnp.concatenate(
        [own[t, 2 * HALF :, :].astype(F32) for t in range(TP) for _ in range(BLK // 2)], axis=0
    )
    info[...] = facts
    eye = iota((TOK, TOK), 0) == iota((TOK, TOK), 1)
    id0, id1 = (
        jnp.sum(jnp.where(eye, facts[:, n : n + 1], 0.0), axis=0, keepdims=True) for n in range(2)
    )
    token, place = iota((ROWS, TOK), 1), iota((ROWS, TOK), 0)
    same, chip, t, i = parts_of(token, place)
    expert = (chip // 2).astype(F32)
    chosen = jnp.where((id0 == expert) | (id1 == expert), 1.0, 0.0)
    earlier = dot(chosen.astype(BF16), before(iota((TOK, TOK), 0), iota((TOK, TOK), 1)))
    kept = jnp.where(same, chosen, 0.0)
    for r in range(2):
        pick[r] = jnp.where(earlier == float(r), kept, 0.0).astype(BF16)
    pick[2] = jnp.where(is_mine(tp[0], same, chip, t, i), 1.0, 0.0).astype(BF16)
    for group in copies[1:]:
        for c in group:
            c.wait()


def send_kernel(pick, group, out, here, sems):
    for b in range(ROWS // 256):
        part = jnp.concatenate(
            [dot(pick[r, 256 * b : 256 * (b + 1), :], group[...]) for r in range(SLOTS)], axis=1
        )
        send_rows(part, here, out, 256 * b, sems.at[b])
    for b in range(ROWS // 256):
        send_wait(here, out, 256 * b, sems.at[b])


def split3(a):
    p1 = a.astype(BF16)
    rest = a - p1.astype(F32)
    p2 = rest.astype(BF16)
    return p1, p2, (rest - p2.astype(F32)).astype(BF16)


def mix_kernel(group, mix_gate, mix):
    block = (iota((TOK, 1), 0) // 4) % BLK
    gates = mix_gate[...].astype(F32)
    gate_rows = jnp.zeros((TOK, 128), F32)
    for k in range(BLK):
        gate_rows = jnp.where(block == k, gates[k : k + 1, :], gate_rows)
    part = jnp.sum(group[...].astype(F32) * gate_rows, axis=1, keepdims=True)
    part = jnp.broadcast_to(part, (TOK, 128))
    a, b = iota((TOK, TOK), 0), iota((TOK, TOK), 1)
    mates = ((a // 32 == b // 32) & (a % 4 == b % 4)).astype(F32).astype(BF16)
    total = sum(dot(mates, p) for p in split3(part))
    mix[...] = 1.0 / (1.0 + jnp.exp(-total))


def weigh_kernel(tp, info, mix, combine):
    facts = info[...]
    id0, id1 = facts[:, 0:1], facts[:, 1:2]
    w0, w1 = facts[:, 2:3] + facts[:, 3:4], facts[:, 4:5] + facts[:, 5:6]
    token, place = iota((TOK, ROWS), 0), iota((TOK, ROWS), 1)
    same, chip, t, i = parts_of(token, place)
    expert = (chip // 2).astype(F32)
    is0, is1 = id0 == expert, id1 == expert
    chosen = jnp.where(is0 | is1, 1.0, 0.0)
    earlier = dot(before(iota((TOK, TOK), 1), iota((TOK, TOK), 0)), chosen.astype(BF16))
    weight = jnp.where(same & (chosen > 0.5), jnp.where(is0, w0, w1), 0.0)
    mine = is_mine(tp[0], same, chip, t, i)
    for r in range(SLOTS):
        if r < 2:
            total = jnp.where(earlier == float(r), weight, 0.0)
        else:
            total = jnp.where(mine, mix[:, 0:1], 0.0)
        high = total.astype(BF16)
        combine[0, r] = high
        combine[1, r] = (total - high.astype(F32)).astype(BF16)


def rows_copy(here, out, first, sem):
    part = slice(first, first + 256)
    return pltpu.make_async_copy(here.at[part, :], out.at[part, :], sem)


def send_rows(values, here, out, first, sem):
    here[first : first + 256, :] = values.astype(BF16)
    rows_copy(here, out, first, sem).start()


def send_wait(here, out, first, sem):
    rows_copy(here, out, first, sem).wait()


def expert_kernel(x, own_hbm, sib, dense_own, dense_sib, out, own, here, sems):
    step = PACK // 8
    copies = [
        pltpu.make_async_copy(
            own_hbm.at[k * step : (k + 1) * step, :], own.at[k * step : (k + 1) * step, :], sems.at[k]
        )
        for k in range(8)
    ]
    for c in copies:
        c.start()

    def place(dim):
        n = iota((256, 256), dim)
        return n % 32 * BLK + n // 32

    order = (iota((256, 256), 1) == place(0)).astype(F32).astype(BF16)
    back = (iota((256, 256), 0) == place(1)).astype(F32).astype(BF16)
    blocks = ROWS // 256
    xs, xd = [], []
    for b in range(blocks):
        y = dot(order, x[256 * b : 256 * (b + 1), :]).astype(BF16)
        for r in range(SLOTS):
            row = jnp.concatenate(
                [y[32 * k : 32 * (k + 1), 128 * r : 128 * (r + 1)] for k in range(BLK)], axis=1
            )
            (xs if r < 2 else xd).append(row)
    xs, xd = jnp.concatenate(xs, axis=0), jnp.concatenate(xd, axis=0)

    def hidden(g, u):
        return (g / (1.0 + jnp.exp(-g)) * u).astype(BF16)

    total = None
    for w in (sib, own):
        if w is own:
            for c in copies:
                c.wait()
        h = hidden(dot(xs, w[0:D, :]), dot(xs, w[D : 2 * D, :]))
        part = jnp.concatenate(
            [dot(h, w[2 * D + 256 * j : 2 * D + 256 * (j + 1), :]) for j in range(4)], axis=1
        )
        total = part if total is None else total + part

    def stack(base):
        parts = [
            ref[DENSE_ROWS * n + base : DENSE_ROWS * n + base + 32, :]
            for ref in (dense_own, dense_sib)
            for n in range(3)
        ]
        for w in (own, sib):
            first = EXPERT_ROWS + base
            parts.append(
                jnp.concatenate(
                    [w[first + DENSE_ROWS * j : first + DENSE_ROWS * j + 32, :] for j in range(4)],
                    axis=1,
                )
            )
        return jnp.concatenate(parts, axis=0)

    h_dense = hidden(dot_t(xd, stack(0)), dot_t(xd, stack(32)))
    dense = dot(h_dense, stack(64)).astype(BF16)
    total = total.astype(BF16)
    for b in range(blocks):
        rows = [total[64 * b : 64 * b + 32], total[64 * b + 32 : 64 * b + 64], dense[32 * b : 32 * b + 32]]
        part = jnp.concatenate(
            [
                jnp.concatenate([a[:, 128 * k : 128 * (k + 1)] for a in rows], axis=1)
                for k in range(BLK)
            ],
            axis=0,
        )
        send_rows(dot(back, part), here, out, 256 * b, sems.at[8 + b])
    for b in range(blocks):
        send_wait(here, out, 256 * b, sems.at[8 + b])


def combine_kernel(combine, returned, out):
    total = None
    for r in range(SLOTS):
        got = returned[:, 128 * r : 128 * (r + 1)]
        part = dot(combine[0, r], got) + dot(combine[1, r], got)
        total = part if total is None else total + part
    out[...] = total.astype(BF16)


def finish_kernel(residual, parts, out):
    total = parts[0].astype(F32)
    for t in range(1, TP):
        total = total + parts[t].astype(F32)
    total = jnp.concatenate([total[4 * k : 4 * (k + 1), :] for k in range(BLK)], axis=1)
    out[...] = (residual[...].astype(F32) + total).astype(BF16)


def in_hbm(array):
    return pltpu.with_memory_space_constraint(array, pltpu.HBM)


def in_vmem(array):
    return pltpu.with_memory_space_constraint(array, pltpu.VMEM)


def shape(*dims, dtype=BF16):
    return jax.ShapeDtypeStruct(dims, dtype)


def a2a(array, axis):
    return lax.all_to_all(array, axis, split_axis=0, concat_axis=0, tiled=True)


def swap(array, axis):
    return lax.ppermute(array, axis, [(i, i ^ 1) for i in range(lax.axis_size(axis))])


def body(
    tokens,
    gain_attn,
    gain_ffn,
    w_query,
    w_key,
    w_value,
    w_output,
    head_bias,
    keys_cache,
    values_cache,
    lengths,
    dense_gate_w,
    dense_up_w,
    dense_down_w,
    mix_gate,
    expert_gate,
    expert_up,
    expert_down,
    routes,
    route_weights,
):
    core = lax.axis_index("c").astype(jnp.int32).reshape(1)
    tp = lax.axis_index("x").astype(jnp.int32).reshape(1)
    wlen = 2 * HALF + 8
    packed, dense_own = call(
        pack_kernel,
        (pltpu.HBM((TP, wlen, 128), BF16), pltpu.HBM((DENSE_ROWS, D), BF16)),
        [SMEM] + [HBM] * 7,
        [
            pltpu.VMEM((2, OWN), jnp.int32),
            pltpu.VMEM((2, OWN), F32),
            pltpu.VMEM((wlen, 128), BF16),
            pltpu.VMEM((DENSE_ROWS, D), BF16),
            pltpu.SemaphoreType.DMA((15,)),
        ],
        outs=HBM,
    )(
        core,
        in_hbm(w_query),
        in_hbm(w_output),
        in_hbm(routes.T),
        in_hbm(route_weights.T),
        in_hbm(dense_gate_w),
        in_hbm(dense_up_w),
        in_hbm(dense_down_w),
    )
    w_own = a2a(packed, "x")
    w_sib = swap(w_own, "c")
    dense_y = swap(dense_own, "y")
    dense_z = swap(dense_own, "z")
    both = [(n, n ^ 9) for n in range(CHIPS)]
    dense_v = lax.ppermute(dense_own, ("z", "y"), both)
    dense_three = call(join_kernel, shape(3 * DENSE_ROWS, D), [VMEM] * 3)(dense_y, dense_z, dense_v)
    expert_own = call(
        expert_pack_kernel,
        pltpu.HBM((PACK, 256), BF16),
        [HBM] * 4,
        [pltpu.VMEM((PACK, 256), BF16), pltpu.SemaphoreType.DMA((2, 12))],
        outs=HBM,
    )(
        in_hbm(expert_gate[0]),
        in_hbm(expert_up[0]),
        in_hbm(expert_down[0]),
        in_hbm(dense_own),
    )
    expert_sib = swap(expert_own, "c")
    dense_three_sib = swap(dense_three, "c")
    attn_in = call(norm_kernel, shape(OWN, D), [VMEM] * 2)(tokens, gain_attn.reshape(1, D))
    new_keys, new_values = call(
        kv_kernel, (shape(OWN, 128), shape(OWN, 128)), [VMEM] * 3
    )(attn_in, w_key, w_value)
    cache = pltpu.VMEM((OWN, CACHE, 128), BF16)
    pick, info, w_here, keys, values = call(
        table_kernel,
        (
            shape(SLOTS, ROWS, TOK),
            shape(TOK, 128, dtype=F32),
            pltpu.VMEM((TP, wlen, 128), BF16),
            cache,
            cache,
        ),
        [SMEM, HBM, HBM, HBM],
        [pltpu.SemaphoreType.DMA((3, OWN))],
    )(tp, in_hbm(w_own), in_hbm(keys_cache), in_hbm(values_cache))
    residual, sent = call(
        attend_kernel, (shape(OWN, D), shape(TP, 32, 128)), [SMEM, SMEM] + [VMEM] * 8
    )(
        core,
        lengths,
        tokens,
        attn_in,
        in_vmem(w_here),
        in_vmem(w_sib),
        head_bias.reshape(1, HEADS),
        in_vmem(keys),
        in_vmem(values),
        gain_ffn.reshape(1, D),
    )
    group = a2a(sent, "x")
    group = group.reshape(TOK, 128)
    rows = call(
        send_kernel,
        pltpu.HBM((ROWS, WIDE), BF16),
        [VMEM] * 2,
        [pltpu.VMEM((ROWS, WIDE), BF16), pltpu.SemaphoreType.DMA((2,))],
        outs=HBM,
    )(pick, group)
    mix = call(mix_kernel, shape(TOK, 128, dtype=F32), [VMEM] * 2)(
        group, mix_gate.reshape(BLK, 128)
    )
    combine = call(
        weigh_kernel, shape(2, SLOTS, TOK, ROWS), [SMEM, VMEM, VMEM], limit=8
    )(tp, info, mix)
    received = a2a(rows.reshape(CHIPS, MSG, WIDE), ("z", "y"))
    sources = (expert_sib,)
    fetched = call(
        fetch_kernel, (pltpu.VMEM((PACK, 256), BF16),), [HBM], [pltpu.SemaphoreType.DMA((1, 4))]
    )(*(in_hbm(a) for a in sources))
    outs = call(
        expert_kernel,
        pltpu.HBM((ROWS, WIDE), BF16),
        [VMEM, HBM] + [VMEM] * 3,
        [
            pltpu.VMEM((PACK, 256), BF16),
            pltpu.VMEM((ROWS, WIDE), BF16),
            pltpu.SemaphoreType.DMA((10,)),
        ],
        16,
        HBM,
    )(received.reshape(ROWS, WIDE), in_hbm(expert_own), *(in_vmem(a) for a in (*fetched, dense_three, dense_three_sib)))
    returned = a2a(outs.reshape(CHIPS, MSG, WIDE), ("z", "y"))
    partial = call(combine_kernel, shape(TOK, 128), [VMEM] * 2)(
        combine, returned.reshape(ROWS, WIDE)
    )
    parts = a2a(partial.reshape(TP, 32, 128), "x")
    layer_out = call(finish_kernel, shape(OWN, D), [VMEM] * 2)(residual, parts)
    return (layer_out, new_keys, new_values)


def solution(mesh):
    grid = Mesh(mesh.devices.reshape(8, 8, 2, TP), ("z", "y", "c", "x"))
    ep = ("z", "y", "c")
    every = ("z", "y", "c", "x")
    return jax.shard_map(
        body,
        mesh=grid,
        in_specs=(
            P(every, None),
            P(),
            P(),
            P(None, "x"),
            P(),
            P(),
            P("x", None),
            P(),
            P(every, None, None),
            P(every, None, None),
            P(every),
            P(ep, None),
            P(ep, None),
            P(ep, None),
            P(),
            P(ep, None, "x"),
            P(ep, None, "x"),
            P(ep, "x", None),
            P(every, None),
            P(every, None),
        ),
        out_specs=(P(every, None), P(every, None), P(every, None)),
        check_vma=False,
    )
```

```python
import math

import jax
import jax.numpy as jnp
from jax import lax
from jax.experimental import pallas as pl
from jax.experimental.pallas import tpu as pltpu
from jax.sharding import Mesh, PartitionSpec as P


HEADS = 8
KV = 2
HEAD = 64
EPS = 1e-06
D = 1024
HALF = D // 2
CACHE = 1024
OWN = 4
TP = 4
CHIPS = 64
MSG = 8
BLK = 8
SLOTS = 3
WIDE = SLOTS * 128
TOK = TP * BLK * 4
ROWS = CHIPS * MSG
F32 = jnp.float32
BF16 = jnp.bfloat16


VMEM = pl.BlockSpec(memory_space=pltpu.VMEM)
SMEM = pl.BlockSpec(memory_space=pltpu.SMEM)
HBM = pl.BlockSpec(memory_space=pltpu.HBM)
EXPERT_ROWS = 3 * D
DENSE_ROWS = 96
PACK = EXPERT_ROWS + 4 * DENSE_ROWS


def dot(a, b):
    return lax.dot_general(a, b, (((1,), (0,)), ((), ())), preferred_element_type=F32)


def dot_t(a, b):
    return lax.dot_general(a, b, (((1,), (1,)), ((), ())), preferred_element_type=F32)


def iota(shape, dim):
    return lax.broadcasted_iota(jnp.int32, shape, dim)


def call(kernel, out_shape, specs, scratch=(), limit=4, outs=VMEM):
    outs = jax.tree.map(lambda _: outs, out_shape)
    return pl.pallas_call(
        kernel,
        out_shape=out_shape,
        in_specs=specs,
        out_specs=outs,
        scratch_shapes=list(scratch),
        compiler_params=pltpu.CompilerParams(vmem_limit_bytes=limit * 1024 * 1024),
    )


def rms(values, gains):
    wide = values.astype(F32)
    scale = lax.rsqrt(jnp.mean(wide * wide, axis=-1, keepdims=True) + EPS)
    return (wide * scale) * gains.astype(F32)


def pack_kernel(
    core, wq, wo, routes_hbm, weights_hbm, gate, up, down, out, dense, routes, weights, half, rows, sems
):
    start = core[0] * HALF
    facts = [
        pltpu.make_async_copy(routes_hbm, routes, sems.at[0]),
        pltpu.make_async_copy(weights_hbm, weights, sems.at[1]),
    ]
    reads = [(wq.at[pl.ds(pl.multiple_of(start, HALF), HALF), :], half.at[0:HALF, :])]
    for j in range(4):
        block = wo.at[:, pl.ds(pl.multiple_of(start + j * 128, 128), 128)]
        reads.append((block, half.at[HALF + 128 * j : HALF + 128 * (j + 1), :]))
    reads = [pltpu.make_async_copy(a, b, sems.at[2 + k]) for k, (a, b) in enumerate(reads)]
    shared = [
        pltpu.make_async_copy(ref, rows.at[32 * k : 32 * (k + 1), :], sems.at[7 + k])
        for k, ref in enumerate((gate, up, down))
    ]
    for c in facts + reads + shared:
        c.start()
    for c in facts:
        c.wait()
    eye = iota((OWN, OWN), 0) == iota((OWN, OWN), 1)

    def column(row):
        return jnp.sum(jnp.where(eye, row, 0.0), axis=1, keepdims=True)

    ids, wts = routes[...].astype(F32), weights[...]
    high = wts.astype(BF16).astype(F32)
    low = wts - high
    lane = iota((OWN, 128), 1)
    info = jnp.zeros((OWN, 128), F32)
    for place, row in enumerate((ids[0:1], ids[1:2], high[0:1], low[0:1], high[1:2], low[1:2])):
        info = jnp.where(lane == place, column(row), info)
    half[2 * HALF : 2 * HALF + 8, :] = jnp.concatenate([info, info], axis=0).astype(BF16)
    for c in reads:
        c.wait()
    sends = [pltpu.make_async_copy(half, out.at[d], sems.at[10 + d]) for d in range(TP)]
    for c in sends:
        c.start()
    for c in shared:
        c.wait()
    last = pltpu.make_async_copy(rows, dense, sems.at[14])
    last.start()
    for c in sends:
        c.wait()
    last.wait()


def norm_kernel(tokens, gain, attn_in):
    attn_in[...] = rms(tokens[...], gain[...]).astype(BF16)


def kv_kernel(attn_in, wk, wv, new_k, new_v):
    a = attn_in[...]
    new_k[...] = dot(a, wk[...]).astype(BF16)
    new_v[...] = dot(a, wv[...]).astype(BF16)


def expert_pack_kernel(gate, up, down, dense, out, here, sems):
    reads = [
        (ref.at[h * HALF : (h + 1) * HALF, :], D * k + HALF * h, HALF)
        for k, ref in enumerate((gate, up))
        for h in range(2)
    ]
    base = 2 * D
    for ref in (down, dense):
        n = ref.shape[0]
        for j in range(4):
            reads.append((ref.at[:, 256 * j : 256 * (j + 1)], base, n))
            base = base + n
    ins, outs = [], []
    for k, (src, first, n) in enumerate(reads):
        place = here.at[first : first + n, :]
        ins.append(pltpu.make_async_copy(src, place, sems.at[0, k]))
        outs.append(pltpu.make_async_copy(place, out.at[first : first + n, :], sems.at[1, k]))
    for c in ins:
        c.start()
    for a, b in zip(ins, outs):
        a.wait()
        b.start()
    for c in outs:
        c.wait()


def join_kernel(a, b, c, out):
    for n, ref in enumerate((a, b, c)):
        out[DENSE_ROWS * n : DENSE_ROWS * (n + 1), :] = ref[...]


def fetch_kernel(*refs):
    n = (len(refs) - 1) // 2
    sems = refs[-1]
    copies = []
    for k in range(n):
        rows = refs[k].shape[0]
        step = rows // 4
        for q in range(4):
            part = slice(q * step, (q + 1) * step)
            copies.append(
                pltpu.make_async_copy(
                    refs[k].at[part, :], refs[n + k].at[part, :], sems.at[k, q]
                )
            )
    for c in copies:
        c.start()
    for c in copies:
        c.wait()


def attend_kernel(
    core, lengths, tokens, attn_in, w_own, w_sib, bias, keys, values, gain, residual, sent
):
    first = core[0] == 0

    def ordered(a, b):
        return jnp.where(first, a, b)

    a = attn_in[...].astype(F32)
    x_own = ordered(a[:, :HALF], a[:, HALF:]).astype(BF16)
    x_sib = ordered(a[:, HALF:], a[:, :HALF]).astype(BF16)
    q = sum(
        dot(a, jnp.concatenate([w[t, 0:HALF, :] for t in range(TP)], axis=1))
        for a, w in ((x_own, w_own), (x_sib, w_sib))
    )
    q = q.astype(BF16).astype(F32)
    head_mask = iota((HEADS, HEADS * HEAD), 1) // HEAD == iota((HEADS, HEADS * HEAD), 0)
    spread = jnp.concatenate(
        [
            jnp.where(head_mask, jnp.broadcast_to(q[b : b + 1], (HEADS, HEADS * HEAD)), 0.0)
            for b in range(OWN)
        ],
        axis=0,
    ).astype(BF16)
    source = iota((HEADS * HEAD, 128), 0)
    fold = (
        (source // (HEADS * HEAD // KV)) * HEAD + source % HEAD == iota((HEADS * HEAD, 128), 1)
    ).astype(F32)
    fold = fold.astype(BF16)
    q_blocks = dot(spread, fold).astype(BF16)
    position = iota((HEADS, CACHE), 1)
    eye = iota((HEADS, HEADS), 0) == iota((HEADS, HEADS), 1)
    offset = jnp.sum(jnp.where(eye, bias[...], 0.0), axis=1, keepdims=True)
    logs, skips, lives = [], [], []
    for b in range(OWN):
        s = dot_t(q_blocks[8 * b : 8 * b + 8], keys[b])
        s = s * (1.0 / math.sqrt(HEAD)) + offset
        tail = jnp.log1p(jnp.exp(-jnp.abs(s)))
        live = position < lengths[b]
        logs.append(jnp.minimum(s, 0.0) - tail)
        skips.append(jnp.where(live, jnp.minimum(-s, 0.0) - tail, 0.0))
        lives.append(live)
    chunks = CACHE // 128
    stacked = jnp.concatenate(
        [skips[b][:, 128 * k : 128 * k + 128] for b in range(OWN) for k in range(chunks)], axis=0
    )
    after = (iota((128, 128), 0) > iota((128, 128), 1)).astype(F32).astype(BF16)
    p1 = stacked.astype(BF16)
    rest = stacked - p1.astype(F32)
    p2 = rest.astype(BF16)
    p3 = (rest - p2.astype(F32)).astype(BF16)
    inner = dot(p1, after) + dot(p2, after) + dot(p3, after)
    totals = jnp.sum(stacked, axis=1, keepdims=True)
    mixes = []
    for b in range(OWN):
        carry = jnp.zeros((HEADS, 1), F32)
        later = [None] * chunks
        for k in reversed(range(chunks)):
            row = 8 * (b * chunks + k)
            later[k] = inner[row : row + 8] + carry
            carry = carry + totals[row : row + 8]
        later = jnp.concatenate(later, axis=1)
        weights = jnp.where(lives[b], jnp.exp(logs[b] + later), 0.0).astype(BF16)
        mixes.append(dot(weights, values[b]))
    mixed = jnp.concatenate(mixes, axis=0).astype(BF16)
    wide = dot_t(mixed, fold)
    mixed = jnp.concatenate(
        [
            jnp.sum(jnp.where(head_mask, wide[8 * b : 8 * b + 8], 0.0), axis=0, keepdims=True)
            for b in range(OWN)
        ],
        axis=0,
    ).astype(BF16)

    def project(w):
        rows = [
            jnp.concatenate([w[t, HALF + 128 * j : HALF + 128 * (j + 1), :] for j in range(4)], axis=1)
            for t in range(TP)
        ]
        return dot(mixed, jnp.concatenate(rows, axis=0))

    out_own, out_sib = project(w_own), project(w_sib)
    total = jnp.concatenate([ordered(out_own, out_sib), ordered(out_sib, out_own)], axis=1)
    res = (tokens[...].astype(F32) + total).astype(BF16)
    residual[...] = res
    f = rms(res, gain[...])
    f = jnp.concatenate([f[:, 128 * k : 128 * (k + 1)] for k in range(BLK)], axis=0).astype(BF16)
    for d in range(TP):
        sent[d] = f


def parts_of(token, place):
    same = (token // 4) % BLK == place % BLK
    chip = place // BLK
    return same, chip, token // 32, token % 4


def is_mine(tp, same, chip, t, i):
    return same & (t == tp) & (i == 2 * ((chip // 8) % 2) + chip % 2)


def before(first, second):
    return (
        ((first // 4) % BLK == 0) & (first // 32 * 4 + first % 4 < second // 32 * 4 + second % 4)
    ).astype(F32).astype(BF16)


def table_kernel(tp, own_hbm, keys_hbm, values_hbm, pick, info, own, keys, values, sems):
    copies = [
        [pltpu.make_async_copy(src.at[b], dst.at[b], sems.at[k, b]) for b in range(OWN)]
        for k, (src, dst) in enumerate(((own_hbm, own), (keys_hbm, keys), (values_hbm, values)))
    ]
    for group in copies:
        for c in group:
            c.start()
    for c in copies[0]:
        c.wait()
    facts = jnp.concatenate(
        [own[t, 2 * HALF :, :].astype(F32) for t in range(TP) for _ in range(BLK // 2)], axis=0
    )
    info[...] = facts
    eye = iota((TOK, TOK), 0) == iota((TOK, TOK), 1)
    id0, id1 = (
        jnp.sum(jnp.where(eye, facts[:, n : n + 1], 0.0), axis=0, keepdims=True) for n in range(2)
    )
    token, place = iota((ROWS, TOK), 1), iota((ROWS, TOK), 0)
    same, chip, t, i = parts_of(token, place)
    expert = (chip // 2).astype(F32)
    chosen = jnp.where((id0 == expert) | (id1 == expert), 1.0, 0.0)
    earlier = dot(chosen.astype(BF16), before(iota((TOK, TOK), 0), iota((TOK, TOK), 1)))
    kept = jnp.where(same, chosen, 0.0)
    for r in range(2):
        pick[r] = jnp.where(earlier == float(r), kept, 0.0).astype(BF16)
    pick[2] = jnp.where(is_mine(tp[0], same, chip, t, i), 1.0, 0.0).astype(BF16)
    for group in copies[1:]:
        for c in group:
            c.wait()


def send_kernel(pick, group, out, here, sems):
    for b in range(ROWS // 256):
        part = jnp.concatenate(
            [dot(pick[r, 256 * b : 256 * (b + 1), :], group[...]) for r in range(SLOTS)], axis=1
        )
        send_rows(part, here, out, 256 * b, sems.at[b])
    for b in range(ROWS // 256):
        send_wait(here, out, 256 * b, sems.at[b])


def split3(a):
    p1 = a.astype(BF16)
    rest = a - p1.astype(F32)
    p2 = rest.astype(BF16)
    return p1, p2, (rest - p2.astype(F32)).astype(BF16)


def mix_kernel(group, mix_gate, mix):
    block = (iota((TOK, 1), 0) // 4) % BLK
    gates = mix_gate[...].astype(F32)
    gate_rows = jnp.zeros((TOK, 128), F32)
    for k in range(BLK):
        gate_rows = jnp.where(block == k, gates[k : k + 1, :], gate_rows)
    part = jnp.sum(group[...].astype(F32) * gate_rows, axis=1, keepdims=True)
    part = jnp.broadcast_to(part, (TOK, 128))
    a, b = iota((TOK, TOK), 0), iota((TOK, TOK), 1)
    mates = ((a // 32 == b // 32) & (a % 4 == b % 4)).astype(F32).astype(BF16)
    total = sum(dot(mates, p) for p in split3(part))
    mix[...] = 1.0 / (1.0 + jnp.exp(-total))


def weigh_kernel(tp, info, mix, combine):
    facts = info[...]
    id0, id1 = facts[:, 0:1], facts[:, 1:2]
    w0, w1 = facts[:, 2:3] + facts[:, 3:4], facts[:, 4:5] + facts[:, 5:6]
    token, place = iota((TOK, ROWS), 0), iota((TOK, ROWS), 1)
    same, chip, t, i = parts_of(token, place)
    expert = (chip // 2).astype(F32)
    is0, is1 = id0 == expert, id1 == expert
    chosen = jnp.where(is0 | is1, 1.0, 0.0)
    earlier = dot(before(iota((TOK, TOK), 1), iota((TOK, TOK), 0)), chosen.astype(BF16))
    weight = jnp.where(same & (chosen > 0.5), jnp.where(is0, w0, w1), 0.0)
    mine = is_mine(tp[0], same, chip, t, i)
    for r in range(SLOTS):
        if r < 2:
            total = jnp.where(earlier == float(r), weight, 0.0)
        else:
            total = jnp.where(mine, mix[:, 0:1], 0.0)
        high = total.astype(BF16)
        combine[0, r] = high
        combine[1, r] = (total - high.astype(F32)).astype(BF16)


def rows_copy(here, out, first, sem):
    part = slice(first, first + 256)
    return pltpu.make_async_copy(here.at[part, :], out.at[part, :], sem)


def send_rows(values, here, out, first, sem):
    here[first : first + 256, :] = values.astype(BF16)
    rows_copy(here, out, first, sem).start()


def send_wait(here, out, first, sem):
    rows_copy(here, out, first, sem).wait()


def expert_kernel(x, own_hbm, sib, dense_own, dense_sib, out, own, here, sems):
    edges = [EXPERT_ROWS, PACK], [0, HALF], [HALF, D], [D, D + HALF], [D + HALF, 2 * D]
    edges = (*edges, [2 * D, 2 * D + HALF], [2 * D + HALF, EXPERT_ROWS])
    copies = [
        pltpu.make_async_copy(own_hbm.at[lo:hi, :], own.at[lo:hi, :], sems.at[k])
        for k, (lo, hi) in enumerate(edges)
    ]
    for c in copies:
        c.start()

    def place(dim):
        n = iota((256, 256), dim)
        return n % 32 * BLK + n // 32

    order = (iota((256, 256), 1) == place(0)).astype(F32).astype(BF16)
    back = (iota((256, 256), 0) == place(1)).astype(F32).astype(BF16)
    blocks = ROWS // 256
    xs, xd = [], []
    for b in range(blocks):
        y = dot(order, x[256 * b : 256 * (b + 1), :]).astype(BF16)
        for r in range(SLOTS):
            row = jnp.concatenate(
                [y[32 * k : 32 * (k + 1), 128 * r : 128 * (r + 1)] for k in range(BLK)], axis=1
            )
            (xs if r < 2 else xd).append(row)
    xs, xd = jnp.concatenate(xs, axis=0), jnp.concatenate(xd, axis=0)

    def hidden(g, u):
        return (g / (1.0 + jnp.exp(-g)) * u).astype(BF16)

    def down(h, w):
        return jnp.concatenate(
            [dot(h, w[2 * D + 256 * j : 2 * D + 256 * (j + 1), :]) for j in range(4)], axis=1
        )

    def stack(base):
        parts = [
            ref[DENSE_ROWS * n + base : DENSE_ROWS * n + base + 32, :]
            for ref in (dense_own, dense_sib)
            for n in range(3)
        ]
        for w in (own, sib):
            first = EXPERT_ROWS + base
            parts.append(
                jnp.concatenate(
                    [w[first + DENSE_ROWS * j : first + DENSE_ROWS * j + 32, :] for j in range(4)],
                    axis=1,
                )
            )
        return jnp.concatenate(parts, axis=0)

    total = down(hidden(dot(xs, sib[0:D, :]), dot(xs, sib[D : 2 * D, :])), sib)
    copies[0].wait()
    h_dense = hidden(dot_t(xd, stack(0)), dot_t(xd, stack(32)))
    dense = dot(h_dense, stack(64)).astype(BF16)
    for c in copies[1:3]:
        c.wait()
    g = dot(xs, own[0:D, :])
    for c in copies[3:5]:
        c.wait()
    h = hidden(g, dot(xs, own[D : 2 * D, :]))
    for c in copies[5:7]:
        c.wait()
    total = total + down(h, own)
    total = total.astype(BF16)
    for b in range(blocks):
        rows = [total[64 * b : 64 * b + 32], total[64 * b + 32 : 64 * b + 64], dense[32 * b : 32 * b + 32]]
        part = jnp.concatenate(
            [
                jnp.concatenate([a[:, 128 * k : 128 * (k + 1)] for a in rows], axis=1)
                for k in range(BLK)
            ],
            axis=0,
        )
        send_rows(dot(back, part), here, out, 256 * b, sems.at[8 + b])
    for b in range(blocks):
        send_wait(here, out, 256 * b, sems.at[8 + b])


def combine_kernel(combine, returned, out):
    total = None
    for r in range(SLOTS):
        got = returned[:, 128 * r : 128 * (r + 1)]
        part = dot(combine[0, r], got) + dot(combine[1, r], got)
        total = part if total is None else total + part
    out[...] = total.astype(BF16)


def finish_kernel(residual, parts, out):
    total = parts[0].astype(F32)
    for t in range(1, TP):
        total = total + parts[t].astype(F32)
    total = jnp.concatenate([total[4 * k : 4 * (k + 1), :] for k in range(BLK)], axis=1)
    out[...] = (residual[...].astype(F32) + total).astype(BF16)


def in_hbm(array):
    return pltpu.with_memory_space_constraint(array, pltpu.HBM)


def in_vmem(array):
    return pltpu.with_memory_space_constraint(array, pltpu.VMEM)


def shape(*dims, dtype=BF16):
    return jax.ShapeDtypeStruct(dims, dtype)


def a2a(array, axis):
    return lax.all_to_all(array, axis, split_axis=0, concat_axis=0, tiled=True)


def swap(array, axis):
    return lax.ppermute(array, axis, [(i, i ^ 1) for i in range(lax.axis_size(axis))])


def body(
    tokens,
    gain_attn,
    gain_ffn,
    w_query,
    w_key,
    w_value,
    w_output,
    head_bias,
    keys_cache,
    values_cache,
    lengths,
    dense_gate_w,
    dense_up_w,
    dense_down_w,
    mix_gate,
    expert_gate,
    expert_up,
    expert_down,
    routes,
    route_weights,
):
    core = lax.axis_index("c").astype(jnp.int32).reshape(1)
    tp = lax.axis_index("x").astype(jnp.int32).reshape(1)
    wlen = 2 * HALF + 8
    packed, dense_own = call(
        pack_kernel,
        (pltpu.HBM((TP, wlen, 128), BF16), pltpu.HBM((DENSE_ROWS, D), BF16)),
        [SMEM] + [HBM] * 7,
        [
            pltpu.VMEM((2, OWN), jnp.int32),
            pltpu.VMEM((2, OWN), F32),
            pltpu.VMEM((wlen, 128), BF16),
            pltpu.VMEM((DENSE_ROWS, D), BF16),
            pltpu.SemaphoreType.DMA((15,)),
        ],
        outs=HBM,
    )(
        core,
        in_hbm(w_query),
        in_hbm(w_output),
        in_hbm(routes.T),
        in_hbm(route_weights.T),
        in_hbm(dense_gate_w),
        in_hbm(dense_up_w),
        in_hbm(dense_down_w),
    )
    w_own = a2a(packed, "x")
    w_sib = swap(w_own, "c")
    dense_y = swap(dense_own, "y")
    dense_z = swap(dense_own, "z")
    both = [(n, n ^ 9) for n in range(CHIPS)]
    dense_v = lax.ppermute(dense_own, ("z", "y"), both)
    dense_three = call(join_kernel, shape(3 * DENSE_ROWS, D), [VMEM] * 3)(dense_y, dense_z, dense_v)
    expert_own = call(
        expert_pack_kernel,
        pltpu.HBM((PACK, 256), BF16),
        [HBM] * 4,
        [pltpu.VMEM((PACK, 256), BF16), pltpu.SemaphoreType.DMA((2, 12))],
        outs=HBM,
    )(
        in_hbm(expert_gate[0]),
        in_hbm(expert_up[0]),
        in_hbm(expert_down[0]),
        in_hbm(dense_own),
    )
    expert_sib = swap(expert_own, "c")
    dense_three_sib = swap(dense_three, "c")
    attn_in = call(norm_kernel, shape(OWN, D), [VMEM] * 2)(tokens, gain_attn.reshape(1, D))
    new_keys, new_values = call(
        kv_kernel, (shape(OWN, 128), shape(OWN, 128)), [VMEM] * 3
    )(attn_in, w_key, w_value)
    cache = pltpu.VMEM((OWN, CACHE, 128), BF16)
    pick, info, w_here, keys, values = call(
        table_kernel,
        (
            shape(SLOTS, ROWS, TOK),
            shape(TOK, 128, dtype=F32),
            pltpu.VMEM((TP, wlen, 128), BF16),
            cache,
            cache,
        ),
        [SMEM, HBM, HBM, HBM],
        [pltpu.SemaphoreType.DMA((3, OWN))],
    )(tp, in_hbm(w_own), in_hbm(keys_cache), in_hbm(values_cache))
    residual, sent = call(
        attend_kernel, (shape(OWN, D), shape(TP, 32, 128)), [SMEM, SMEM] + [VMEM] * 8
    )(
        core,
        lengths,
        tokens,
        attn_in,
        in_vmem(w_here),
        in_vmem(w_sib),
        head_bias.reshape(1, HEADS),
        in_vmem(keys),
        in_vmem(values),
        gain_ffn.reshape(1, D),
    )
    group = a2a(sent, "x")
    group = group.reshape(TOK, 128)
    rows = call(
        send_kernel,
        pltpu.HBM((ROWS, WIDE), BF16),
        [VMEM] * 2,
        [pltpu.VMEM((ROWS, WIDE), BF16), pltpu.SemaphoreType.DMA((2,))],
        outs=HBM,
    )(pick, group)
    mix = call(mix_kernel, shape(TOK, 128, dtype=F32), [VMEM] * 2)(
        group, mix_gate.reshape(BLK, 128)
    )
    combine = call(
        weigh_kernel, shape(2, SLOTS, TOK, ROWS), [SMEM, VMEM, VMEM], limit=8
    )(tp, info, mix)
    received = a2a(rows.reshape(CHIPS, MSG, WIDE), ("z", "y"))
    sources = (expert_sib,)
    fetched = call(
        fetch_kernel, (pltpu.VMEM((PACK, 256), BF16),), [HBM], [pltpu.SemaphoreType.DMA((1, 4))]
    )(*(in_hbm(a) for a in sources))
    outs = call(
        expert_kernel,
        pltpu.HBM((ROWS, WIDE), BF16),
        [VMEM, HBM] + [VMEM] * 3,
        [
            pltpu.VMEM((PACK, 256), BF16),
            pltpu.VMEM((ROWS, WIDE), BF16),
            pltpu.SemaphoreType.DMA((10,)),
        ],
        16,
        HBM,
    )(received.reshape(ROWS, WIDE), in_hbm(expert_own), *(in_vmem(a) for a in (*fetched, dense_three, dense_three_sib)))
    returned = a2a(outs.reshape(CHIPS, MSG, WIDE), ("z", "y"))
    partial = call(combine_kernel, shape(TOK, 128), [VMEM] * 2)(
        combine, returned.reshape(ROWS, WIDE)
    )
    parts = a2a(partial.reshape(TP, 32, 128), "x")
    layer_out = call(finish_kernel, shape(OWN, D), [VMEM] * 2)(residual, parts)
    return (layer_out, new_keys, new_values)


def solution(mesh):
    grid = Mesh(mesh.devices.reshape(8, 8, 2, TP), ("z", "y", "c", "x"))
    ep = ("z", "y", "c")
    every = ("z", "y", "c", "x")
    return jax.shard_map(
        body,
        mesh=grid,
        in_specs=(
            P(every, None),
            P(),
            P(),
            P(None, "x"),
            P(),
            P(),
            P("x", None),
            P(),
            P(every, None, None),
            P(every, None, None),
            P(every),
            P(ep, None),
            P(ep, None),
            P(ep, None),
            P(),
            P(ep, None, "x"),
            P(ep, None, "x"),
            P(ep, "x", None),
            P(every, None),
            P(every, None),
        ),
        out_specs=(P(every, None), P(every, None), P(every, None)),
        check_vma=False,
    )
```

```python
import math

import jax
import jax.numpy as jnp
from jax import lax
from jax.experimental import pallas as pl
from jax.experimental.pallas import tpu as pltpu
from jax.sharding import Mesh, PartitionSpec as P


HEADS = 8
KV = 2
HEAD = 64
EPS = 1e-06
D = 1024
HALF = D // 2
CACHE = 1024
OWN = 4
TP = 4
CHIPS = 64
MSG = 8
BLK = 8
SLOTS = 3
WIDE = SLOTS * 128
TOK = TP * BLK * 4
ROWS = CHIPS * MSG
F32 = jnp.float32
BF16 = jnp.bfloat16


VMEM = pl.BlockSpec(memory_space=pltpu.VMEM)
SMEM = pl.BlockSpec(memory_space=pltpu.SMEM)
HBM = pl.BlockSpec(memory_space=pltpu.HBM)
EXPERT_ROWS = 3 * D
DENSE_ROWS = 96
PACK = EXPERT_ROWS + 4 * DENSE_ROWS


def dot(a, b):
    return lax.dot_general(a, b, (((1,), (0,)), ((), ())), preferred_element_type=F32)


def dot_t(a, b):
    return lax.dot_general(a, b, (((1,), (1,)), ((), ())), preferred_element_type=F32)


def iota(shape, dim):
    return lax.broadcasted_iota(jnp.int32, shape, dim)


def call(kernel, out_shape, specs, scratch=(), limit=4, outs=VMEM):
    outs = jax.tree.map(lambda _: outs, out_shape)
    return pl.pallas_call(
        kernel,
        out_shape=out_shape,
        in_specs=specs,
        out_specs=outs,
        scratch_shapes=list(scratch),
        compiler_params=pltpu.CompilerParams(vmem_limit_bytes=limit * 1024 * 1024),
    )


def rms(values, gains):
    wide = values.astype(F32)
    scale = lax.rsqrt(jnp.mean(wide * wide, axis=-1, keepdims=True) + EPS)
    return (wide * scale) * gains.astype(F32)


def pack_kernel(
    core, wq, wo, routes_hbm, weights_hbm, gate, up, down, out, dense, routes, weights, half, rows, sems
):
    start = core[0] * HALF
    facts = [
        pltpu.make_async_copy(routes_hbm, routes, sems.at[0]),
        pltpu.make_async_copy(weights_hbm, weights, sems.at[1]),
    ]
    reads = [(wq.at[pl.ds(pl.multiple_of(start, HALF), HALF), :], half.at[0:HALF, :])]
    for j in range(4):
        block = wo.at[:, pl.ds(pl.multiple_of(start + j * 128, 128), 128)]
        reads.append((block, half.at[HALF + 128 * j : HALF + 128 * (j + 1), :]))
    reads = [pltpu.make_async_copy(a, b, sems.at[2 + k]) for k, (a, b) in enumerate(reads)]
    shared = [
        pltpu.make_async_copy(ref, rows.at[32 * k : 32 * (k + 1), :], sems.at[7 + k])
        for k, ref in enumerate((gate, up, down))
    ]
    for c in facts + reads + shared:
        c.start()
    for c in facts:
        c.wait()
    eye = iota((OWN, OWN), 0) == iota((OWN, OWN), 1)

    def column(row):
        return jnp.sum(jnp.where(eye, row, 0.0), axis=1, keepdims=True)

    ids, wts = routes[...].astype(F32), weights[...]
    high = wts.astype(BF16).astype(F32)
    low = wts - high
    lane = iota((OWN, 128), 1)
    info = jnp.zeros((OWN, 128), F32)
    for place, row in enumerate((ids[0:1], ids[1:2], high[0:1], low[0:1], high[1:2], low[1:2])):
        info = jnp.where(lane == place, column(row), info)
    half[2 * HALF : 2 * HALF + 8, :] = jnp.concatenate([info, info], axis=0).astype(BF16)
    for c in reads:
        c.wait()
    sends = [pltpu.make_async_copy(half, out.at[d], sems.at[10 + d]) for d in range(TP)]
    for c in sends:
        c.start()
    for c in shared:
        c.wait()
    last = pltpu.make_async_copy(rows, dense, sems.at[14])
    last.start()
    for c in sends:
        c.wait()
    last.wait()


def norm_kernel(tokens, gain, attn_in):
    attn_in[...] = rms(tokens[...], gain[...]).astype(BF16)


def kv_kernel(attn_in, wk, wv, new_k, new_v):
    a = attn_in[...]
    new_k[...] = dot(a, wk[...]).astype(BF16)
    new_v[...] = dot(a, wv[...]).astype(BF16)


def expert_pack_kernel(gate, up, down, dense, out, here, sems):
    reads = [
        (ref.at[h * HALF : (h + 1) * HALF, :], D * k + HALF * h, HALF)
        for k, ref in enumerate((gate, up))
        for h in range(2)
    ]
    base = 2 * D
    for ref in (down, dense):
        n = ref.shape[0]
        for j in range(4):
            reads.append((ref.at[:, 256 * j : 256 * (j + 1)], base, n))
            base = base + n
    ins, outs = [], []
    for k, (src, first, n) in enumerate(reads):
        place = here.at[first : first + n, :]
        ins.append(pltpu.make_async_copy(src, place, sems.at[0, k]))
        outs.append(pltpu.make_async_copy(place, out.at[first : first + n, :], sems.at[1, k]))
    for c in ins:
        c.start()
    for a, b in zip(ins, outs):
        a.wait()
        b.start()
    for c in outs:
        c.wait()


def join_kernel(a, b, c, out):
    for n, ref in enumerate((a, b, c)):
        out[DENSE_ROWS * n : DENSE_ROWS * (n + 1), :] = ref[...]


def attend_kernel(
    core, lengths, tokens, attn_in, w_own, w_sib, bias, keys, values, gain, residual, sent
):
    first = core[0] == 0

    def ordered(a, b):
        return jnp.where(first, a, b)

    a = attn_in[...].astype(F32)
    x_own = ordered(a[:, :HALF], a[:, HALF:]).astype(BF16)
    x_sib = ordered(a[:, HALF:], a[:, :HALF]).astype(BF16)
    q = sum(
        dot(a, jnp.concatenate([w[t, 0:HALF, :] for t in range(TP)], axis=1))
        for a, w in ((x_own, w_own), (x_sib, w_sib))
    )
    q = q.astype(BF16).astype(F32)
    head_mask = iota((HEADS, HEADS * HEAD), 1) // HEAD == iota((HEADS, HEADS * HEAD), 0)
    spread = jnp.concatenate(
        [
            jnp.where(head_mask, jnp.broadcast_to(q[b : b + 1], (HEADS, HEADS * HEAD)), 0.0)
            for b in range(OWN)
        ],
        axis=0,
    ).astype(BF16)
    source = iota((HEADS * HEAD, 128), 0)
    fold = (
        (source // (HEADS * HEAD // KV)) * HEAD + source % HEAD == iota((HEADS * HEAD, 128), 1)
    ).astype(F32)
    fold = fold.astype(BF16)
    q_blocks = dot(spread, fold).astype(BF16)
    position = iota((HEADS, CACHE), 1)
    eye = iota((HEADS, HEADS), 0) == iota((HEADS, HEADS), 1)
    offset = jnp.sum(jnp.where(eye, bias[...], 0.0), axis=1, keepdims=True)
    logs, skips, lives = [], [], []
    for b in range(OWN):
        s = dot_t(q_blocks[8 * b : 8 * b + 8], keys[b])
        s = s * (1.0 / math.sqrt(HEAD)) + offset
        tail = jnp.log1p(jnp.exp(-jnp.abs(s)))
        live = position < lengths[b]
        logs.append(jnp.minimum(s, 0.0) - tail)
        skips.append(jnp.where(live, jnp.minimum(-s, 0.0) - tail, 0.0))
        lives.append(live)
    chunks = CACHE // 128
    stacked = jnp.concatenate(
        [skips[b][:, 128 * k : 128 * k + 128] for b in range(OWN) for k in range(chunks)], axis=0
    )
    after = (iota((128, 128), 0) > iota((128, 128), 1)).astype(F32).astype(BF16)
    p1 = stacked.astype(BF16)
    rest = stacked - p1.astype(F32)
    p2 = rest.astype(BF16)
    p3 = (rest - p2.astype(F32)).astype(BF16)
    inner = dot(p1, after) + dot(p2, after) + dot(p3, after)
    totals = jnp.sum(stacked, axis=1, keepdims=True)
    mixes = []
    for b in range(OWN):
        carry = jnp.zeros((HEADS, 1), F32)
        later = [None] * chunks
        for k in reversed(range(chunks)):
            row = 8 * (b * chunks + k)
            later[k] = inner[row : row + 8] + carry
            carry = carry + totals[row : row + 8]
        later = jnp.concatenate(later, axis=1)
        weights = jnp.where(lives[b], jnp.exp(logs[b] + later), 0.0).astype(BF16)
        mixes.append(dot(weights, values[b]))
    mixed = jnp.concatenate(mixes, axis=0).astype(BF16)
    wide = dot_t(mixed, fold)
    mixed = jnp.concatenate(
        [
            jnp.sum(jnp.where(head_mask, wide[8 * b : 8 * b + 8], 0.0), axis=0, keepdims=True)
            for b in range(OWN)
        ],
        axis=0,
    ).astype(BF16)

    def project(w):
        rows = [
            jnp.concatenate([w[t, HALF + 128 * j : HALF + 128 * (j + 1), :] for j in range(4)], axis=1)
            for t in range(TP)
        ]
        return dot(mixed, jnp.concatenate(rows, axis=0))

    out_own, out_sib = project(w_own), project(w_sib)
    total = jnp.concatenate([ordered(out_own, out_sib), ordered(out_sib, out_own)], axis=1)
    res = (tokens[...].astype(F32) + total).astype(BF16)
    residual[...] = res
    f = rms(res, gain[...])
    f = jnp.concatenate([f[:, 128 * k : 128 * (k + 1)] for k in range(BLK)], axis=0).astype(BF16)
    for d in range(TP):
        sent[d] = f


def parts_of(token, place):
    same = (token // 4) % BLK == place % BLK
    chip = place // BLK
    return same, chip, token // 32, token % 4


def is_mine(tp, same, chip, t, i):
    return same & (t == tp) & (i == 2 * ((chip // 8) % 2) + chip % 2)


def before(first, second):
    return (
        ((first // 4) % BLK == 0) & (first // 32 * 4 + first % 4 < second // 32 * 4 + second % 4)
    ).astype(F32).astype(BF16)


def table_kernel(tp, own_hbm, keys_hbm, values_hbm, pick, info, own, keys, values, sems):
    copies = [
        [pltpu.make_async_copy(src.at[b], dst.at[b], sems.at[k, b]) for b in range(OWN)]
        for k, (src, dst) in enumerate(((own_hbm, own), (keys_hbm, keys), (values_hbm, values)))
    ]
    for group in copies:
        for c in group:
            c.start()
    for c in copies[0]:
        c.wait()
    facts = jnp.concatenate(
        [own[t, 2 * HALF :, :].astype(F32) for t in range(TP) for _ in range(BLK // 2)], axis=0
    )
    info[...] = facts
    eye = iota((TOK, TOK), 0) == iota((TOK, TOK), 1)
    id0, id1 = (
        jnp.sum(jnp.where(eye, facts[:, n : n + 1], 0.0), axis=0, keepdims=True) for n in range(2)
    )
    token, place = iota((ROWS, TOK), 1), iota((ROWS, TOK), 0)
    same, chip, t, i = parts_of(token, place)
    expert = (chip // 2).astype(F32)
    chosen = jnp.where((id0 == expert) | (id1 == expert), 1.0, 0.0)
    earlier = dot(chosen.astype(BF16), before(iota((TOK, TOK), 0), iota((TOK, TOK), 1)))
    kept = jnp.where(same, chosen, 0.0)
    for r in range(2):
        pick[r] = jnp.where(earlier == float(r), kept, 0.0).astype(BF16)
    pick[2] = jnp.where(is_mine(tp[0], same, chip, t, i), 1.0, 0.0).astype(BF16)
    for group in copies[1:]:
        for c in group:
            c.wait()


def send_kernel(pick, group, out, here, sems):
    for b in range(ROWS // 256):
        part = jnp.concatenate(
            [dot(pick[r, 256 * b : 256 * (b + 1), :], group[...]) for r in range(SLOTS)], axis=1
        )
        send_rows(part, here, out, 256 * b, sems.at[b])
    for b in range(ROWS // 256):
        send_wait(here, out, 256 * b, sems.at[b])


def split3(a):
    p1 = a.astype(BF16)
    rest = a - p1.astype(F32)
    p2 = rest.astype(BF16)
    return p1, p2, (rest - p2.astype(F32)).astype(BF16)


def mix_kernel(group, mix_gate, mix):
    block = (iota((TOK, 1), 0) // 4) % BLK
    gates = mix_gate[...].astype(F32)
    gate_rows = jnp.zeros((TOK, 128), F32)
    for k in range(BLK):
        gate_rows = jnp.where(block == k, gates[k : k + 1, :], gate_rows)
    part = jnp.sum(group[...].astype(F32) * gate_rows, axis=1, keepdims=True)
    part = jnp.broadcast_to(part, (TOK, 128))
    a, b = iota((TOK, TOK), 0), iota((TOK, TOK), 1)
    mates = ((a // 32 == b // 32) & (a % 4 == b % 4)).astype(F32).astype(BF16)
    total = sum(dot(mates, p) for p in split3(part))
    mix[...] = 1.0 / (1.0 + jnp.exp(-total))


def weigh_kernel(tp, info, mix, combine):
    facts = info[...]
    id0, id1 = facts[:, 0:1], facts[:, 1:2]
    w0, w1 = facts[:, 2:3] + facts[:, 3:4], facts[:, 4:5] + facts[:, 5:6]
    token, place = iota((TOK, ROWS), 0), iota((TOK, ROWS), 1)
    same, chip, t, i = parts_of(token, place)
    expert = (chip // 2).astype(F32)
    is0, is1 = id0 == expert, id1 == expert
    chosen = jnp.where(is0 | is1, 1.0, 0.0)
    earlier = dot(before(iota((TOK, TOK), 1), iota((TOK, TOK), 0)), chosen.astype(BF16))
    weight = jnp.where(same & (chosen > 0.5), jnp.where(is0, w0, w1), 0.0)
    mine = is_mine(tp[0], same, chip, t, i)
    for r in range(SLOTS):
        if r < 2:
            total = jnp.where(earlier == float(r), weight, 0.0)
        else:
            total = jnp.where(mine, mix[:, 0:1], 0.0)
        high = total.astype(BF16)
        combine[0, r] = high
        combine[1, r] = (total - high.astype(F32)).astype(BF16)


def rows_copy(here, out, first, sem):
    part = slice(first, first + 256)
    return pltpu.make_async_copy(here.at[part, :], out.at[part, :], sem)


def send_rows(values, here, out, first, sem):
    here[first : first + 256, :] = values.astype(BF16)
    rows_copy(here, out, first, sem).start()


def send_wait(here, out, first, sem):
    rows_copy(here, out, first, sem).wait()


def expert_kernel(x, own_hbm, sib, dense_own, dense_sib, out, own, here, sems):
    edges = [EXPERT_ROWS, PACK], [0, HALF], [HALF, D], [D, D + HALF], [D + HALF, 2 * D]
    edges = (*edges, [2 * D, 2 * D + HALF], [2 * D + HALF, EXPERT_ROWS])
    copies = [
        pltpu.make_async_copy(own_hbm.at[lo:hi, :], own.at[lo:hi, :], sems.at[k])
        for k, (lo, hi) in enumerate(edges)
    ]
    for c in copies:
        c.start()

    def place(dim):
        n = iota((256, 256), dim)
        return n % 32 * BLK + n // 32

    order = (iota((256, 256), 1) == place(0)).astype(F32).astype(BF16)
    back = (iota((256, 256), 0) == place(1)).astype(F32).astype(BF16)
    blocks = ROWS // 256
    xs, xd = [], []
    for b in range(blocks):
        y = dot(order, x[256 * b : 256 * (b + 1), :]).astype(BF16)
        for r in range(SLOTS):
            row = jnp.concatenate(
                [y[32 * k : 32 * (k + 1), 128 * r : 128 * (r + 1)] for k in range(BLK)], axis=1
            )
            (xs if r < 2 else xd).append(row)
    xs, xd = jnp.concatenate(xs, axis=0), jnp.concatenate(xd, axis=0)

    def hidden(g, u):
        return (g / (1.0 + jnp.exp(-g)) * u).astype(BF16)

    def down(h, w):
        return jnp.concatenate(
            [dot(h, w[2 * D + 256 * j : 2 * D + 256 * (j + 1), :]) for j in range(4)], axis=1
        )

    def stack(base):
        parts = [
            ref[DENSE_ROWS * n + base : DENSE_ROWS * n + base + 32, :]
            for ref in (dense_own, dense_sib)
            for n in range(3)
        ]
        for w in (own, sib):
            first = EXPERT_ROWS + base
            parts.append(
                jnp.concatenate(
                    [w[first + DENSE_ROWS * j : first + DENSE_ROWS * j + 32, :] for j in range(4)],
                    axis=1,
                )
            )
        return jnp.concatenate(parts, axis=0)

    total = down(hidden(dot(xs, sib[0:D, :]), dot(xs, sib[D : 2 * D, :])), sib)
    copies[0].wait()
    h_dense = hidden(dot_t(xd, stack(0)), dot_t(xd, stack(32)))
    dense = dot(h_dense, stack(64)).astype(BF16)
    for c in copies[1:3]:
        c.wait()
    g = dot(xs, own[0:D, :])
    for c in copies[3:5]:
        c.wait()
    h = hidden(g, dot(xs, own[D : 2 * D, :]))
    for c in copies[5:7]:
        c.wait()
    total = total + down(h, own)
    total = total.astype(BF16)
    for b in range(blocks):
        rows = [total[64 * b : 64 * b + 32], total[64 * b + 32 : 64 * b + 64], dense[32 * b : 32 * b + 32]]
        part = jnp.concatenate(
            [
                jnp.concatenate([a[:, 128 * k : 128 * (k + 1)] for a in rows], axis=1)
                for k in range(BLK)
            ],
            axis=0,
        )
        send_rows(dot(back, part), here, out, 256 * b, sems.at[8 + b])
    for b in range(blocks):
        send_wait(here, out, 256 * b, sems.at[8 + b])


def combine_kernel(combine, returned, out):
    total = None
    for r in range(SLOTS):
        got = returned[:, 128 * r : 128 * (r + 1)]
        part = dot(combine[0, r], got) + dot(combine[1, r], got)
        total = part if total is None else total + part
    out[...] = total.astype(BF16)


def finish_kernel(residual, parts, out):
    total = parts[0].astype(F32)
    for t in range(1, TP):
        total = total + parts[t].astype(F32)
    total = jnp.concatenate([total[4 * k : 4 * (k + 1), :] for k in range(BLK)], axis=1)
    out[...] = (residual[...].astype(F32) + total).astype(BF16)


def in_hbm(array):
    return pltpu.with_memory_space_constraint(array, pltpu.HBM)


def in_vmem(array):
    return pltpu.with_memory_space_constraint(array, pltpu.VMEM)


def shape(*dims, dtype=BF16):
    return jax.ShapeDtypeStruct(dims, dtype)


def a2a(array, axis):
    return lax.all_to_all(array, axis, split_axis=0, concat_axis=0, tiled=True)


def swap(array, axis):
    return lax.ppermute(array, axis, [(i, i ^ 1) for i in range(lax.axis_size(axis))])


def body(
    tokens,
    gain_attn,
    gain_ffn,
    w_query,
    w_key,
    w_value,
    w_output,
    head_bias,
    keys_cache,
    values_cache,
    lengths,
    dense_gate_w,
    dense_up_w,
    dense_down_w,
    mix_gate,
    expert_gate,
    expert_up,
    expert_down,
    routes,
    route_weights,
):
    core = lax.axis_index("c").astype(jnp.int32).reshape(1)
    tp = lax.axis_index("x").astype(jnp.int32).reshape(1)
    wlen = 2 * HALF + 8
    packed, dense_own = call(
        pack_kernel,
        (pltpu.HBM((TP, wlen, 128), BF16), pltpu.HBM((DENSE_ROWS, D), BF16)),
        [SMEM] + [HBM] * 7,
        [
            pltpu.VMEM((2, OWN), jnp.int32),
            pltpu.VMEM((2, OWN), F32),
            pltpu.VMEM((wlen, 128), BF16),
            pltpu.VMEM((DENSE_ROWS, D), BF16),
            pltpu.SemaphoreType.DMA((15,)),
        ],
        outs=HBM,
    )(
        core,
        in_hbm(w_query),
        in_hbm(w_output),
        in_hbm(routes.T),
        in_hbm(route_weights.T),
        in_hbm(dense_gate_w),
        in_hbm(dense_up_w),
        in_hbm(dense_down_w),
    )
    w_own = a2a(packed, "x")
    w_sib = swap(w_own, "c")
    dense_y = swap(dense_own, "y")
    dense_z = swap(dense_own, "z")
    both = [(n, n ^ 9) for n in range(CHIPS)]
    dense_v = lax.ppermute(dense_own, ("z", "y"), both)
    dense_three = call(join_kernel, shape(3 * DENSE_ROWS, D), [VMEM] * 3)(dense_y, dense_z, dense_v)
    expert_own = call(
        expert_pack_kernel,
        pltpu.HBM((PACK, 256), BF16),
        [HBM] * 4,
        [pltpu.VMEM((PACK, 256), BF16), pltpu.SemaphoreType.DMA((2, 12))],
        outs=HBM,
    )(
        in_hbm(expert_gate[0]),
        in_hbm(expert_up[0]),
        in_hbm(expert_down[0]),
        in_hbm(dense_own),
    )
    expert_sib = swap(expert_own, "c")
    dense_three_sib = swap(dense_three, "c")
    attn_in = call(norm_kernel, shape(OWN, D), [VMEM] * 2)(tokens, gain_attn.reshape(1, D))
    new_keys, new_values = call(
        kv_kernel, (shape(OWN, 128), shape(OWN, 128)), [VMEM] * 3
    )(attn_in, w_key, w_value)
    cache = pltpu.VMEM((OWN, CACHE, 128), BF16)
    pick, info, w_here, keys, values = call(
        table_kernel,
        (
            shape(SLOTS, ROWS, TOK),
            shape(TOK, 128, dtype=F32),
            pltpu.VMEM((TP, wlen, 128), BF16),
            cache,
            cache,
        ),
        [SMEM, HBM, HBM, HBM],
        [pltpu.SemaphoreType.DMA((3, OWN))],
    )(tp, in_hbm(w_own), in_hbm(keys_cache), in_hbm(values_cache))
    residual, sent = call(
        attend_kernel, (shape(OWN, D), shape(TP, 32, 128)), [SMEM, SMEM] + [VMEM] * 8
    )(
        core,
        lengths,
        tokens,
        attn_in,
        in_vmem(w_here),
        in_vmem(w_sib),
        head_bias.reshape(1, HEADS),
        in_vmem(keys),
        in_vmem(values),
        gain_ffn.reshape(1, D),
    )
    group = a2a(sent, "x")
    group = group.reshape(TOK, 128)
    rows = call(
        send_kernel,
        pltpu.HBM((ROWS, WIDE), BF16),
        [VMEM] * 2,
        [pltpu.VMEM((ROWS, WIDE), BF16), pltpu.SemaphoreType.DMA((2,))],
        outs=HBM,
    )(pick, group)
    mix = call(mix_kernel, shape(TOK, 128, dtype=F32), [VMEM] * 2)(
        group, mix_gate.reshape(BLK, 128)
    )
    combine = call(
        weigh_kernel, shape(2, SLOTS, TOK, ROWS), [SMEM, VMEM, VMEM], limit=8
    )(tp, info, mix)
    received = a2a(rows.reshape(CHIPS, MSG, WIDE), ("z", "y"))
    outs = call(
        expert_kernel,
        pltpu.HBM((ROWS, WIDE), BF16),
        [VMEM, HBM] + [VMEM] * 3,
        [
            pltpu.VMEM((PACK, 256), BF16),
            pltpu.VMEM((ROWS, WIDE), BF16),
            pltpu.SemaphoreType.DMA((10,)),
        ],
        16,
        HBM,
    )(received.reshape(ROWS, WIDE), in_hbm(expert_own), *(in_vmem(a) for a in (expert_sib, dense_three, dense_three_sib)))
    returned = a2a(outs.reshape(CHIPS, MSG, WIDE), ("z", "y"))
    partial = call(combine_kernel, shape(TOK, 128), [VMEM] * 2)(
        combine, returned.reshape(ROWS, WIDE)
    )
    parts = a2a(partial.reshape(TP, 32, 128), "x")
    layer_out = call(finish_kernel, shape(OWN, D), [VMEM] * 2)(residual, parts)
    return (layer_out, new_keys, new_values)


def solution(mesh):
    grid = Mesh(mesh.devices.reshape(8, 8, 2, TP), ("z", "y", "c", "x"))
    ep = ("z", "y", "c")
    every = ("z", "y", "c", "x")
    return jax.shard_map(
        body,
        mesh=grid,
        in_specs=(
            P(every, None),
            P(),
            P(),
            P(None, "x"),
            P(),
            P(),
            P("x", None),
            P(),
            P(every, None, None),
            P(every, None, None),
            P(every),
            P(ep, None),
            P(ep, None),
            P(ep, None),
            P(),
            P(ep, None, "x"),
            P(ep, None, "x"),
            P(ep, "x", None),
            P(every, None),
            P(every, None),
        ),
        out_specs=(P(every, None), P(every, None), P(every, None)),
        check_vma=False,
    )
```
